32 devices in a mesh: sp: 8 (over z, x), tp: 4 (over y, core).
Axes of the slice: x: 2, y: 2, z: 4, core: 2. Of those that a mesh axis runs over, the one named last changes fastest.
Arguments:
- block_input: bfloat16 [16384, 4096], P('sp'), may hold values from -6 to 6
- value_weight: bfloat16 [4096, 1024], P(None, 'tp'), may hold values from -0.09375 to 0.09375
- key_rows: bfloat16 [16384, 512], P('sp', 'tp'), may hold values from -1 to 1
- query_rows: bfloat16 [16384, 512], P('sp', 'tp'), may hold values from -1 to 1
- decay_pre: float32 [16, 16384], P('tp', 'sp'), may hold values from -3 to 2
- decay_log: float32 [16], P('tp'), may hold values from -16 to -2
- gate_rows: bfloat16 [16384, 1024], P('sp', 'tp'), may hold values from -6 to 6
- out_grad: bfloat16 [16384, 1024], P('sp', 'tp'), may hold values from -6 to 6
Outputs:
- key_grad: float32 [16384, 512], P('sp', 'tp')
- query_grad: float32 [16384, 512], P('sp', 'tp')
- decay_grad: float32 [16, 16384], P('tp', 'sp')
- gate_grad: float32 [16384, 1024], P('sp', 'tp')
- weight_grad: float32 [4096, 1024], P('sp', 'tp')
- row_norms: float32 [4096], P('sp')
The draws below stay inside these ranges and needn't reach their ends.
All inputs are finite; a program needn't handle non-finite values.
Results may differ from the reference program's by a relative error of at most 0.0035.
Values sent between devices are 32-bit elements; how exact they have to be, the bound alone decides.
A program may use at most 128 MiB of HBM per device.

```python
import jax
import jax.numpy as jnp
from jax import lax

D = 4096
HEADS = 16
HEAD = 64
GROUPS = 8
STATE = 64
BLK = 128
TOK_DEV = 2048
TOKENS = 16384


def draw_decay_log(key, part):
    pick_key, slow_key, fast_key = jax.random.split(jax.random.fold_in(key, 11), 3)
    slow_share = 0.5
    is_slow = jax.random.uniform(pick_key, (HEADS,), jnp.float32) < slow_share
    slow_rate = jax.random.uniform(slow_key, (HEADS,), jnp.float32, 0.25, 0.5) / TOKENS
    fast_rate = jax.random.uniform(fast_key, (HEADS,), jnp.float32, 0.05, 0.1)
    return jnp.log(jnp.where(is_slow, slow_rate, fast_rate)).astype(jnp.float32)


def draw_decay_pre(key, part):
    level_key, noise_key = jax.random.split(jax.random.fold_in(key, 23), 2)
    levels = jax.random.uniform(level_key, (HEADS, TOKENS // TOK_DEV), jnp.float32, -1.5, 1.0)
    noise = jax.random.uniform(noise_key, (HEADS, TOKENS), jnp.float32, -0.99, 0.99)
    return (jnp.repeat(levels, TOK_DEV, axis=1) + noise).astype(jnp.float32)


def raised(array, key, source, target, blocks, factor):
    def block_of(position):
        return (jnp.arange(array.shape[position]) // (array.shape[position] // blocks)).reshape((-1,) + (1,) * (array.ndim - 1 - position))

    one_side = jax.random.permutation(key, blocks)[block_of(target)]
    other_side = (block_of(target) + blocks // 2) % blocks
    return jnp.where((block_of(source) == one_side) | (block_of(source) == other_side), factor * array, array)


def steps_of(stream_key, shape, cuts, least, high):
    factor_of, own = 1.0, jax.random.fold_in(stream_key, 6)
    for dim, shards_of in cuts:
        heights = jnp.exp(jax.random.uniform(jax.random.fold_in(own, dim), (shards_of,), jnp.float32, least / len(cuts), high / len(cuts)))
        factor_of = factor_of * jnp.repeat(heights, shape[dim] // shards_of).reshape([-1 if axis == dim else 1 for axis in range(len(shape))])
    return factor_of


def bell_draw(key, shape, width, most, cuts=(), dtype=jnp.bfloat16):
    level = steps_of(key, shape, cuts, -0.22, 0.18) if cuts else 1.0
    drawn = jax.random.normal(key, shape, jnp.float32) * width * level
    return jnp.minimum(jnp.maximum(drawn, -most), most).astype(dtype)


def noise_with(own_key, dims, scale, most, cuts, heavy, kind=jnp.bfloat16):
    entries = scale * jax.random.normal(own_key, dims, jnp.float32)
    if cuts:
        entries = entries * steps_of(own_key, dims, cuts, -0.22, 0.18)
    return jnp.clip(raised(entries, jax.random.fold_in(own_key, 3), *heavy), -most, most).astype(kind)


def setup_inputs(seed: int = 0) -> dict:
    arg_keys = jax.random.split(jax.random.key(seed), 9)
    return {
        "block_input": noise_with(arg_keys[0], (TOKENS, D), 1.0, 6.0, ((0, 8),), (0, 1, 8, 2.0)),
        "value_weight": bell_draw(arg_keys[1], (D, HEADS * HEAD), D ** -0.5, 0.09375, ((1, 4),)),
        "key_rows": bell_draw(arg_keys[2], (TOKENS, GROUPS * STATE), 0.125, 1.0, ((0, 8), (1, 4))),
        "query_rows": bell_draw(arg_keys[3], (TOKENS, GROUPS * STATE), 0.125, 1.0, ((0, 8), (1, 4))),
        "decay_pre": draw_decay_pre(jax.random.fold_in(arg_keys[8], 71), 0),
        "decay_log": draw_decay_log(jax.random.fold_in(arg_keys[8], 71), 0),
        "gate_rows": bell_draw(arg_keys[6], (TOKENS, HEADS * HEAD), 1.0, 6.0, ((0, 8), (1, 4))),
        "out_grad": bell_draw(arg_keys[7], (TOKENS, HEADS * HEAD), 1.0, 6.0, ((0, 8), (1, 4))),
    }


HIGH = lax.Precision.HIGHEST

def block_mixer(values, key_float, query_float, step_sizes, log_steps, start_state):
    length, head_count, head_width = values.shape
    groups = key_float.shape[1]
    group_ratio = head_count // groups
    blocks = length // BLK
    value_blocks = values.reshape(blocks, BLK, head_count, head_width)
    key_blocks = jnp.repeat(key_float.reshape(blocks, BLK, groups, -1), group_ratio, axis=2)
    query_blocks = jnp.repeat(query_float.reshape(blocks, BLK, groups, -1), group_ratio, axis=2)
    step_blocks = step_sizes.reshape(head_count, blocks, BLK).transpose(1, 0, 2)
    running = jnp.cumsum(log_steps.reshape(head_count, blocks, BLK).transpose(1, 0, 2), axis=-1)
    lower = jnp.tril(jnp.ones((BLK, BLK), bool))
    spread = jnp.where(lower, running[..., :, None] - running[..., None, :], 0.0)
    decay = jnp.where(lower, jnp.exp(spread), 0.0)
    scores = jnp.einsum('cqhn,ckhn->chqk', query_blocks, key_blocks, precision=HIGH)
    weights = scores * decay * step_blocks[:, :, None, :]
    inner = jnp.einsum('chqk,ckhp->cqhp', weights, value_blocks, precision=HIGH)
    to_end = jnp.exp(running[..., -1:] - running) * step_blocks
    block_states = jnp.einsum('cqhn,chq,cqhp->chpn', key_blocks, to_end, value_blocks, precision=HIGH)
    factors = jnp.exp(running[..., -1])

    def advance(state_now, item):
        contrib, factor = item
        return (factor[:, None, None] * state_now + contrib, state_now)
    end_state, before = lax.scan(advance, start_state, (block_states, factors))
    outer = jnp.einsum('cqhn,chpn,chq->cqhp', query_blocks, before, jnp.exp(running), precision=HIGH)
    return ((inner + outer).reshape(length, head_count, head_width), end_state)

def reference(block_input, value_weight, key_rows, query_rows, decay_pre, decay_log, gate_rows, out_grad):
    head_count = decay_log.shape[0]
    length = block_input.shape[0]
    groups = key_rows.shape[1] // STATE
    projected = jnp.dot(block_input, value_weight, preferred_element_type=jnp.float32).astype(jnp.bfloat16)
    pre_float = lax.optimization_barrier(projected).astype(jnp.float32)
    sig_pre = jax.nn.sigmoid(pre_float)
    values = (pre_float * sig_pre).reshape(length, head_count, HEAD)
    step_sizes = jax.nn.softplus(decay_pre)
    decay_rates = jnp.exp(decay_log)
    log_steps = -decay_rates[:, None] * step_sizes
    key_float = key_rows.astype(jnp.float32).reshape(length, groups, STATE)
    query_float = query_rows.astype(jnp.float32).reshape(length, groups, STATE)
    gate_float = gate_rows.astype(jnp.float32)
    sig_gate = jax.nn.sigmoid(gate_float)
    cot_float = out_grad.astype(jnp.float32)
    zero_state = jnp.zeros((head_count, HEAD, STATE), jnp.float32)

    def forward(vals, krows, qrows, sizes, logs):
        mixed, _ = block_mixer(vals, krows, qrows, sizes, logs, zero_state)
        return mixed
    mixed, pullback = jax.vjp(forward, values, key_float, query_float, step_sizes, log_steps)
    grad_mixed = (cot_float * gate_float * sig_gate).reshape(length, head_count, HEAD)
    value_back, key_back, query_back, size_back, log_back = pullback(grad_mixed)
    gate_grad = cot_float * mixed.reshape(length, head_count * HEAD) * sig_gate * (1.0 + gate_float * (1.0 - sig_gate))
    size_total = size_back - decay_rates[:, None] * log_back
    decay_grad = size_total * jax.nn.sigmoid(decay_pre)
    value_grad = (value_back.reshape(length, head_count * HEAD) * sig_pre * (1.0 + pre_float * (1.0 - sig_pre))).astype(jnp.bfloat16)
    weight_grad = lax.dot_general(block_input, value_grad, (((0,), (0,)), ((), ())), preferred_element_type=jnp.float32)
    row_norms = lax.optimization_barrier(jnp.sum(weight_grad * weight_grad, axis=1))
    return (key_back.reshape(length, groups * STATE), query_back.reshape(length, groups * STATE), decay_grad, gate_grad, weight_grad, row_norms)
```

```python
import functools

import jax
import jax.numpy as jnp
from jax import lax
from jax.experimental import pallas as pl
from jax.experimental.pallas import tpu as pltpu
from jax.sharding import PartitionSpec as P

HEAD = 64
STATE = 64
BLK = 128
ROWS = 8
LOADS = 8

BF = jnp.bfloat16
F32 = jnp.float32
MESH = pl.DeviceIdType.MESH


def dot(a, b, ca, cb):
    return lax.dot_general(a, b, (((ca,), (cb,)), ((), ())), preferred_element_type=F32)


def iota(shape, dim):
    return lax.broadcasted_iota(jnp.int32, shape, dim)


def sigmoid(v):
    return 1.0 / (1.0 + jnp.exp(-v))


def thirds(q):
    hi = q.astype(BF).astype(F32)
    rest = q - hi
    mid = rest.astype(BF).astype(F32)
    return jnp.concatenate([hi, mid, rest - mid], axis=0).astype(BF)


def halves(q):
    hi = q.astype(BF)
    return hi, (q - hi.astype(F32)).astype(BF)


def by_blocks(a, count, width):
    if count == 1:
        return a
    lane = iota(a.shape, 1) // width
    return jnp.concatenate([jnp.where(lane == i, a, jnp.zeros_like(a)) for i in range(count)], axis=0)


def kernel(c, x_hbm, w_hbm, key_hbm, query_hbm, pre_ref, log_ref, gate_hbm, out_hbm,
           dkey_hbm, dquery_hbm, ddecay_ref, dgate_hbm, wgrad_hbm, norm_ref,
           xv, wv, kv, qv, gv, ov, run_s, runs_s, step_s, cols_s, grads_s, gfs_s, dstates, states,
           fac_s, after_s, ahead_s, vals_s, te_s, dval_s, vslope_s, vte_s, dgate_s, dkey_s, dquery_s,
           vgt_s, part, xrecv, zbuf, rev_out, rev_in, fwd_out, fwd_in, outgo_s, income_s, wg_s, norms, fac_row,
           in_sem, x_sem, rev_ss, rev_rs, fwd_ss, fwd_rs, xs, xr, zs, zr, ns, nr, o_sem):
    heads, ratio, blocks, n, ntp, X, Z = c["heads"], c["ratio"], c["blocks"], c["n"], c["ntp"], c["X"], c["Z"]
    groups = heads // ratio
    wide, narrow, CD = heads * HEAD, groups * STATE, c["cd"]
    gw = ratio * HEAD
    PC = max(1, blocks // Z)
    PR = wide // PC
    tokens = blocks * BLK
    me, tpi = lax.axis_index("sp"), lax.axis_index("tp")
    z, x = me // X, lax.rem(me, X)

    def local(src, dst, sem):
        return pltpu.make_async_copy(src, dst, sem)

    def remote(src, dst, ssem, rsem, axis, to):
        return pltpu.make_async_remote_copy(src, dst, ssem, rsem, device_id={axis: to}, device_id_type=MESH)

    loads = [local(gate_hbm, gv, in_sem.at[0]), local(out_hbm, ov, in_sem.at[1]),
             local(query_hbm, qv, in_sem.at[2]), local(key_hbm, kv, in_sem.at[3]),
             local(w_hbm, wv, in_sem.at[4])]
    for copy in loads:
        copy.start()
    XR = tokens // LOADS

    def x_load(m):
        rows = pl.ds(pl.multiple_of(m * XR, XR), XR)
        return local(x_hbm.at[rows, :], xv.at[rows, :], x_sem.at[m])

    for m in range(LOADS):
        x_load(m).start()

    barrier = pltpu.get_barrier_semaphore()
    for d in range(1, n):
        pl.semaphore_signal(barrier, inc=1, device_id={"sp": lax.rem(me + d, n)}, device_id_type=MESH)
    for d in range(1, ntp):
        pl.semaphore_signal(barrier, inc=1, device_id={"tp": lax.rem(tpi + d, ntp)}, device_id_type=MESH)

    head_row = iota((ROWS, BLK), 0)
    rate = jnp.zeros((ROWS, BLK), F32)
    for h in range(heads):
        rate = jnp.where(head_row == h, jnp.broadcast_to(log_ref[h], (ROWS, BLK)), rate)
    rate = jnp.where(head_row < heads, jnp.exp(rate), 0.0)
    run_s[...] = jnp.zeros_like(run_s)
    for b in range(blocks):
        run_s[b * ROWS:b * ROWS + heads, :] = pre_ref[:, b * BLK:(b + 1) * BLK]
    pre_all = run_s[...]
    step_all = jnp.maximum(pre_all, 0.0) + jnp.log1p(jnp.exp(-jnp.abs(pre_all)))
    step_s[...] = step_all
    lanes = iota((blocks * ROWS, BLK), 1)
    acc = -jnp.concatenate([rate] * blocks, axis=0) * step_all
    shift = 1
    while shift < BLK:
        acc = acc + jnp.where(lanes >= shift, pltpu.roll(acc, shift, 1), 0.0)
        shift *= 2
    run_s[...] = acc
    runs_all = acc - jnp.log(step_all)
    runs_s[...] = runs_all
    for b in range(blocks):
        rows = slice(b * ROWS, (b + 1) * ROWS)
        cols_s[b * BLK:(b + 1) * BLK, :] = jnp.concatenate([acc[rows], runs_all[rows]], axis=0).T

    spread = jnp.where((iota((3 * ROWS, wide), 0) & (ROWS - 1)) == iota((3 * ROWS, wide), 1) // HEAD,
                       1.0, 0.0).astype(BF)
    own = iota((narrow, wide), 0) // STATE == iota((narrow, wide), 1) // gw
    pick = jnp.where(iota((ROWS, wide), 0) == iota((ROWS, wide), 1) // HEAD, 1.0, 0.0).astype(BF)
    at_row, at_col = iota((BLK, BLK), 0), iota((BLK, BLK), 1)

    def toks(b):
        return pl.ds(pl.multiple_of(b * BLK, BLK), BLK)

    def heads8(b):
        return pl.ds(pl.multiple_of(b * ROWS, ROWS), ROWS)

    def compact(a):
        total = a[0:STATE]
        for g in range(1, groups):
            total = total + a[g * STATE:(g + 1) * STATE]
        return total

    def widen(a):
        return jnp.where(own, jnp.concatenate([a] * groups, axis=0), 0.0)

    dstates[blocks] = jnp.zeros((narrow, wide), F32)
    for copy in loads[:3]:
        copy.wait()

    def reverse(i, decayed):
        b = blocks - 1 - i
        tk = toks(b)
        gate, cot = gv[tk, :].astype(F32), ov[tk, :].astype(F32)
        sig = sigmoid(gate)
        cs = cot * sig
        grads = cs * gate
        grads_s[tk, :] = grads
        dgate_s[tk, :] = cs * (1.0 + gate * (1.0 - sig))
        fs = dot(thirds(jnp.exp(run_s[heads8(b), :])), spread, 0, 0)
        gfs = (grads * fs).astype(BF)
        gfs_s[tk, :] = gfs
        factor = fs[BLK - 1:BLK, :]
        fac_s[b] = jnp.broadcast_to(factor, (ROWS, wide))
        after_s[b] = decayed
        back = dot(qv[tk, :], gfs, 0, 0)
        dstates[b] = dstates[b + 1] * factor + jnp.where(own, back, 0.0)
        return decayed * factor

    decayed = lax.fori_loop(0, blocks, reverse, jnp.ones((ROWS, wide), F32), unroll=2)

    rev_out[0:STATE, :] = compact(dstates[0])
    rev_out[STATE:STATE + ROWS, :] = decayed
    pl.semaphore_wait(barrier, n - 1 + ntp - 1)

    def rev_copy(d):
        return remote(rev_out, rev_in.at[d - 1], rev_ss.at[d - 1], rev_rs.at[d - 1], "sp", lax.rem(me + n - d, n))

    def fwd_copy(d):
        return remote(fwd_out, fwd_in.at[d - 1], fwd_ss.at[d - 1], fwd_rs.at[d - 1], "sp", lax.rem(me + d, n))

    for d in range(1, n):
        @pl.when(me >= d)
        def _(d=d):
            rev_copy(d).start()

    loads[4].wait()

    def project(m, carry):
        x_load(m).wait()
        rows = pl.ds(pl.multiple_of(m * XR, XR), XR)
        gv[rows, :] = jnp.dot(xv[rows, :], wv[...], preferred_element_type=F32).astype(BF)
        return carry

    lax.fori_loop(0, LOADS, project, 0)

    loads[3].wait()
    states[0] = jnp.zeros((narrow, wide), F32)

    def forward(b, before):
        tk = toks(b)
        pre = gv[tk, :].astype(F32)
        sig = sigmoid(pre)
        vals = pre * sig
        vals_s[tk, :] = vals
        vslope_s[tk, :] = sig * (1.0 + pre * (1.0 - sig))
        run, runs = run_s[heads8(b), :], runs_s[heads8(b), :]
        te = dot(thirds(jnp.exp(run[:, BLK - 1:BLK] - runs)), spread, 0, 0)
        te_s[tk, :] = te
        vte = (vals * te).astype(BF)
        vte_s[tk, :] = vte
        key, query = kv[tk, :], qv[tk, :]
        factor = fac_s[b]
        ahead_s[b] = before
        states[b + 1] = states[b] * factor[0:1] + jnp.where(own, dot(key, vte, 0, 0), 0.0)
        scores = dot(key, by_blocks(query, groups, STATE), 1, 1)
        cols = cols_s[tk, :]
        grads = grads_s[tk, :].astype(BF)
        outer = dot(key, dstates[b + 1].astype(BF), 1, 0) * te
        for g in range(groups):
            weights = []
            for h in range(g * ratio, (g + 1) * ratio):
                decay = jnp.exp(jnp.where(at_col >= at_row, run[h:h + 1, :] - cols[:, ROWS + h:ROWS + h + 1], -1e30))
                weights.append((scores[:, g * BLK:(g + 1) * BLK] * decay).astype(BF))
            gs = slice(g * gw, (g + 1) * gw)
            inner = dot(jnp.concatenate(weights, axis=1), by_blocks(grads[:, gs], ratio, HEAD), 1, 0)
            dval_s[tk, gs] = inner + outer[:, gs]
        return before * factor

    decayed = lax.fori_loop(0, blocks, forward, jnp.ones((ROWS, wide), F32), unroll=2)
    fwd_out[0:STATE, :] = compact(states[blocks])
    fwd_out[STATE:STATE + ROWS, :] = decayed
    for d in range(1, n):
        @pl.when(me + d < n)
        def _(d=d):
            fwd_copy(d).start()

    def gather(into, store, copy_of, there):
        into[...] = jnp.zeros_like(into)
        fac_row[...] = jnp.ones_like(fac_row)
        for d in range(1, n):
            @pl.when(there(d))
            def _(d=d):
                copy_of(d).wait_recv()
                into[...] += widen(store[d - 1, 0:STATE, :]) * fac_row[0:1, :]
                fac_row[...] *= store[d - 1, STATE:STATE + ROWS, :]

    gather(outgo_s, rev_in, rev_copy, lambda d: me + d < n)

    def correct(b, carry):
        tk = toks(b)
        extra = (outgo_s[...] * after_s[b][0:1]).astype(BF)
        dval = dval_s[tk, :] + dot(kv[tk, :], extra, 1, 0) * te_s[tk, :]
        dval_s[tk, :] = dval
        vgt_s[:, tk] = (dval * vslope_s[tk, :]).T.astype(BF)
        return carry

    lax.fori_loop(0, blocks, correct, 0, unroll=2)

    def chunk_of(k):
        out = jnp.int32(0)
        for i in range(Z):
            order = sorted(range(Z), key=lambda zc: -abs(zc - i))
            here = jnp.int32(0)
            for kk in range(Z):
                here = jnp.where(k == kk, order[kk], here)
            out = jnp.where(z == i, here, out)
        return out

    def x_copy(t, p):
        rows = pl.ds(pl.multiple_of(p * PR, PR), PR)
        to = z * X + lax.rem(x + 1 + t // Z, X)
        return remote(part.at[t, rows, :], xrecv.at[t, rows, :], xs.at[t * PC + p], xr.at[t * PC + p], "sp", to)

    def chunk(t, carry):
        k = lax.rem(t, Z)
        dest = chunk_of(k) * X + lax.rem(x + 1 + t // Z, X)
        for half in range(max(1, CD // 256)):
            step = min(256, CD)
            cs = pl.ds(pl.multiple_of(dest * CD + half * step, 128), step)
            part[t, :, half * step:(half + 1) * step] = jnp.dot(vgt_s[...], xv[:, cs], preferred_element_type=F32)

        @pl.when(t < (X - 1) * Z)
        def _():
            for p in range(PC):
                x_copy(t, p).start()
        return carry

    lax.fori_loop(0, X * Z, chunk, 0)

    gather(income_s, fwd_in, fwd_copy, lambda d: me >= d)

    def grads_of(b):
        tk = toks(b)
        key, query = kv[tk, :], qv[tk, :]
        grads, vals = grads_s[tk, :], vals_s[tk, :]
        grads_b, vals_b = grads.astype(BF), vals.astype(BF)
        run, runs = run_s[heads8(b), :], runs_s[heads8(b), :]
        cols = cols_s[tk, :]
        before = ahead_s[b][0:1]
        factor = fac_s[b][0:1]
        state = states[b] + before * income_s[...]
        after = states[b + 1] + (before * factor) * income_s[...]
        dstate = dstates[b + 1] + after_s[b][0:1] * outgo_s[...]
        state_b, dstate_b = state.astype(BF), dstate.astype(BF)
        keys = by_blocks(key, groups, STATE)
        scores = dot(query, keys, 1, 1)
        pulled = dot(grads_b, by_blocks(vals_b, heads, HEAD), 1, 1)
        fs = dot(thirds(jnp.exp(run)), spread, 0, 0)
        outer = dot(query, state_b, 1, 0) * fs
        totals = []
        mixed = []
        for g in range(groups):
            weights, total = [], None
            for h in range(g * ratio, (g + 1) * ratio):
                decay = jnp.exp(jnp.where(at_row >= at_col, cols[:, h:h + 1] - runs[h:h + 1, :], -1e30))
                weights.append((scores[:, g * BLK:(g + 1) * BLK] * decay).astype(BF))
                item = pulled[:, h * BLK:(h + 1) * BLK] * decay
                total = item if total is None else total + item
            totals.append(total.astype(BF))
            gs = slice(g * gw, (g + 1) * gw)
            inner = dot(jnp.concatenate(weights, axis=1), by_blocks(vals_b[:, gs], ratio, HEAD), 1, 0)
            mixed.append(inner + outer[:, gs])
        mixed = jnp.concatenate(mixed, axis=1)
        dgate_s[tk, :] = mixed * dgate_s[tk, :]
        total = jnp.concatenate(totals, axis=1)
        dquery_s[tk, :] = dot(gfs_s[tk, :], state_b, 1, 1) + dot(total, keys, 1, 0)
        across = dot(total, query, 0, 0)
        dkey = dot(vte_s[tk, :], dstate_b, 1, 1)
        mine = across[0:BLK]
        for g in range(1, groups):
            mine = jnp.where(iota((BLK, narrow), 1) // STATE == g, across[g * BLK:(g + 1) * BLK], mine)
        dkey_s[tk, :] = dkey + mine
        there = sum(dot(pick, part_, 1, 1) for part_ in halves(grads * mixed))
        here = sum(dot(pick, part_, 1, 1) for part_ in halves(vals * dval_s[tk, :]))
        cross_lanes = jnp.broadcast_to(jnp.sum(after * dstate, axis=0, keepdims=True), (ROWS, wide))
        cross = jnp.sum(jnp.where(iota((ROWS, wide), 0) == iota((ROWS, wide), 1) // HEAD, cross_lanes, 0.0),
                        axis=1, keepdims=True)
        back = there - here
        lane = iota((ROWS, BLK), 1)
        shift = 1
        while shift < BLK:
            back = back + jnp.where(lane < BLK - shift, pltpu.roll(back, BLK - shift, 1), 0.0)
            shift *= 2
        pre = pre_ref[:, tk]
        size_total = (here / step_s[heads8(b), :] - rate * (back + cross))[0:heads]
        ddecay_ref[:, tk] = size_total * sigmoid(pre)

    def z_up(k, p):
        zc = chunk_of(k)
        to = jnp.where(zc < z, z - 1, z + 1)
        slot = jnp.where((zc > z) & (zc == to), Z, zc)
        rows = pl.ds(pl.multiple_of(p * PR, PR), PR)
        return remote(part.at[(X - 1) * Z + k, rows, :], zbuf.at[slot, rows, :], zs.at[k * PC + p],
                      zr.at[slot * PC + p], "sp", lax.rem(to * X + x + n, n))

    def z_arrival(slot, p):
        rows = pl.ds(pl.multiple_of(p * PR, PR), PR)
        other = lax.rem(me + X, n)
        return remote(part.at[0, rows, :], zbuf.at[slot, rows, :], zs.at[p], zr.at[slot * PC + p], "sp", other)

    def reduce(s):
        k, p = s // PC, lax.rem(s, PC)
        zc = chunk_of(k)
        rows = pl.ds(pl.multiple_of(p * PR, PR), PR)
        mine = (X - 1) * Z + k
        total = part[mine, rows, :]
        for xi in range(X - 1):
            x_copy(xi * Z + k, p).wait_recv()
            total = total + xrecv[xi * Z + k, rows, :]
        part[mine, rows, :] = total

        @pl.when(((zc <= z) & (z < Z - 1)) | ((zc > z) & (z > 0)))
        def _():
            z_arrival(zc, p).wait_recv()
            part[mine, rows, :] += zbuf[zc, rows, :]

        @pl.when((zc == z) & (z > 0))
        def _():
            z_arrival(Z, p).wait_recv()
            part[mine, rows, :] += zbuf[Z, rows, :]

        @pl.when(zc != z)
        def _():
            z_up(k, p).start()

    outs = [local(dkey_s, dkey_hbm, o_sem.at[0]), local(dquery_s, dquery_hbm, o_sem.at[1]),
            local(dgate_s, dgate_hbm, o_sem.at[2])]
    pair = 2 if blocks % 2 == 0 else 1

    def both(s, carry):
        for i in range(pair):
            grads_of(pair * s + i)
        reduce(s)
        return carry

    def rest(s, carry):
        reduce(s)
        return carry

    early = blocks // pair
    lax.fori_loop(0, early, both, 0)
    for copy in outs:
        copy.start()
    lax.fori_loop(early, Z * PC, rest, 0)

    last = part[X * Z - 1]
    norms[tpi] = jnp.broadcast_to(jnp.sum(last * last, axis=0, keepdims=True), (ROWS, CD))

    def norm_copy(d):
        return remote(norms.at[tpi], norms.at[tpi], ns.at[d - 1], nr.at[d - 1], "tp", lax.rem(tpi + d, ntp))

    for d in range(1, ntp):
        norm_copy(d).start()
    wg_s[...] = last.T
    wcopy = local(wg_s, wgrad_hbm, o_sem.at[3])
    wcopy.start()

    for d in range(1, n):
        @pl.when(me >= d)
        def _(d=d):
            rev_copy(d).wait_send()

        @pl.when(me + d < n)
        def _(d=d):
            fwd_copy(d).wait_send()

    def sent(t, carry):
        x_copy(t // PC, lax.rem(t, PC)).wait_send()
        return carry

    lax.fori_loop(0, (X - 1) * Z * PC, sent, 0)

    def passed(t, carry):
        z_up(t // PC, lax.rem(t, PC)).wait_send()
        return carry

    lax.fori_loop(0, (Z - 1) * PC, passed, 0)
    for d in range(1, ntp):
        got = remote(norms.at[tpi], norms.at[lax.rem(tpi + ntp - d, ntp)], ns.at[d - 1], nr.at[d - 1], "tp",
                     lax.rem(tpi + d, ntp))
        got.wait()
    total = norms[0]
    for i in range(1, ntp):
        total = total + norms[i]
    norm_ref[...] = total[0:1]
    for copy in outs:
        copy.wait()
    wcopy.wait()


def shards(block_input, value_weight, key_rows, query_rows, decay_pre, decay_log, gate_rows, out_grad):
    heads = decay_log.shape[0]
    tokens, depth = block_input.shape
    groups = key_rows.shape[1] // STATE
    wide, narrow = heads * HEAD, groups * STATE
    blocks = tokens // BLK
    n, ntp = lax.axis_size("sp"), lax.axis_size("tp")
    X = max(1, ntp // 2)
    if n % X:
        X = 1
    Z = n // X
    cd = depth // n
    PC = max(1, blocks // Z)
    c = dict(heads=heads, ratio=heads // groups, blocks=blocks, n=n, ntp=ntp, X=X, Z=Z, cd=cd)
    hbm = pl.BlockSpec(memory_space=pl.ANY)
    vmem = pl.BlockSpec(memory_space=pltpu.VMEM)
    V = pltpu.VMEM
    dma = pltpu.SemaphoreType.DMA
    outs = pl.pallas_call(
        functools.partial(kernel, c),
        in_specs=[hbm, hbm, hbm, hbm, vmem, pl.BlockSpec(memory_space=pltpu.SMEM), hbm, hbm],
        out_specs=[hbm, hbm, vmem, hbm, hbm, vmem],
        out_shape=[
            jax.ShapeDtypeStruct((tokens, narrow), F32),
            jax.ShapeDtypeStruct((tokens, narrow), F32),
            jax.ShapeDtypeStruct((heads, tokens), F32),
            jax.ShapeDtypeStruct((tokens, wide), F32),
            jax.ShapeDtypeStruct((cd, wide), F32),
            jax.ShapeDtypeStruct((1, cd), F32),
        ],
        scratch_shapes=[
            V((tokens, depth), BF), V((depth, wide), BF), V((tokens, narrow), BF), V((tokens, narrow), BF),
            V((tokens, wide), BF), V((tokens, wide), BF),
            V((blocks * ROWS, BLK), F32), V((blocks * ROWS, BLK), F32), V((blocks * ROWS, BLK), F32),
            V((tokens, 2 * ROWS), F32), V((tokens, wide), F32), V((tokens, wide), BF),
            V((blocks + 1, narrow, wide), F32), V((blocks + 1, narrow, wide), F32),
            V((blocks, ROWS, wide), F32), V((blocks, ROWS, wide), F32), V((blocks, ROWS, wide), F32),
            V((tokens, wide), F32), V((tokens, wide), F32), V((tokens, wide), F32), V((tokens, wide), F32),
            V((tokens, wide), BF), V((tokens, wide), F32), V((tokens, narrow), F32), V((tokens, narrow), F32),
            V((wide, tokens), BF), V((X * Z, wide, cd), F32), V((max(1, X - 1) * Z, wide, cd), F32),
            V((Z + 1, wide, cd), F32),
            V((STATE + ROWS, wide), F32), V((n - 1, STATE + ROWS, wide), F32),
            V((STATE + ROWS, wide), F32), V((n - 1, STATE + ROWS, wide), F32),
            V((narrow, wide), F32), V((narrow, wide), F32), V((cd, wide), F32), V((ntp, ROWS, cd), F32),
            V((ROWS, wide), F32),
            dma((5,)), dma((LOADS,)), dma((n - 1,)), dma((n - 1,)), dma((n - 1,)), dma((n - 1,)),
            dma((max(1, X - 1) * Z * PC,)), dma((max(1, X - 1) * Z * PC,)),
            dma((Z * PC,)), dma(((Z + 1) * PC,)), dma((ntp - 1,)), dma((ntp - 1,)), dma((4,)),
        ],
        compiler_params=pltpu.CompilerParams(
            collective_id=0, has_side_effects=True, vmem_limit_bytes=66_000_000),
        name="mixer_back",
    )(block_input, value_weight, key_rows, query_rows, decay_pre, decay_log, gate_rows, out_grad)
    key_grad, query_grad, decay_grad, gate_grad, weight_grad, norm = outs
    return key_grad, query_grad, decay_grad, gate_grad, weight_grad, norm.reshape(cd)


def solution(mesh):
    in_specs = (
        P("sp", None),
        P(None, "tp"),
        P("sp", "tp"),
        P("sp", "tp"),
        P("tp", "sp"),
        P("tp"),
        P("sp", "tp"),
        P("sp", "tp"),
    )
    out_specs = (P("sp", "tp"), P("sp", "tp"), P("tp", "sp"), P("sp", "tp"), P("sp", "tp"), P("sp"))
    return jax.shard_map(shards, mesh=mesh, in_specs=in_specs, out_specs=out_specs, check_vma=False)
```

```python
import functools

import jax
import jax.numpy as jnp
from jax import lax
from jax.experimental import pallas as pl
from jax.experimental.pallas import tpu as pltpu
from jax.sharding import PartitionSpec as P

HEAD = 64
STATE = 64
BLK = 128
ROWS = 8
LOADS = 8
PIECE = 32

BF = jnp.bfloat16
F32 = jnp.float32
MESH = pl.DeviceIdType.MESH


def dot(a, b, ca, cb):
    return lax.dot_general(a, b, (((ca,), (cb,)), ((), ())), preferred_element_type=F32)


def iota(shape, dim):
    return lax.broadcasted_iota(jnp.int32, shape, dim)


def sigmoid(v):
    return 1.0 / (1.0 + jnp.exp(-v))


def thirds(q):
    hi = q.astype(BF).astype(F32)
    rest = q - hi
    mid = rest.astype(BF).astype(F32)
    return jnp.concatenate([hi, mid, rest - mid], axis=0).astype(BF)


def halves(q):
    hi = q.astype(BF)
    return hi, (q - hi.astype(F32)).astype(BF)


def by_blocks(a, count, width):
    if count == 1:
        return a
    lane = iota(a.shape, 1) // width
    return jnp.concatenate([jnp.where(lane == i, a, jnp.zeros_like(a)) for i in range(count)], axis=0)


def kernel(c, x_hbm, w_hbm, key_hbm, query_hbm, pre_ref, log_ref, gate_hbm, out_hbm,
           dkey_hbm, dquery_hbm, ddecay_ref, dgate_hbm, wgrad_hbm, norm_ref,
           xv, wv, kv, qv, gv, ov, run_s, runs_s, step_s, cols_s, grads_s, gfs_s, dstates, states,
           fac_s, after_s, ahead_s, vals_s, te_s, dval_s, vslope_s, vte_s, dgate_s, dkey_s, dquery_s,
           vgt_s, part, xrecv, zbuf, zlast, xlast, row_in, col_out, col_in, outgo_s, income_s, pass_s,
           wg_s, norms,
           in_sem, x_sem, row_ss, row_rs, col_ss, col_rs, xs, xr, zs, zr, zls, zlr, xls, xlr, ns, nr, o_sem):
    heads, ratio, blocks, n, ntp, X, Z = c["heads"], c["ratio"], c["blocks"], c["n"], c["ntp"], c["X"], c["Z"]
    groups = heads // ratio
    wide, narrow, CD = heads * HEAD, groups * STATE, c["cd"]
    gw = ratio * HEAD
    PU = gw // PIECE
    NP = groups * PU
    tokens = blocks * BLK
    me, tpi = lax.axis_index("sp"), lax.axis_index("tp")
    z, x = me // X, lax.rem(me, X)

    def local(src, dst, sem):
        return pltpu.make_async_copy(src, dst, sem)

    def remote(src, dst, ssem, rsem, axis, to):
        return pltpu.make_async_remote_copy(src, dst, ssem, rsem, device_id={axis: to}, device_id_type=MESH)

    loads = [local(gate_hbm, gv, in_sem.at[0]), local(out_hbm, ov, in_sem.at[1]),
             local(query_hbm, qv, in_sem.at[2]), local(key_hbm, kv, in_sem.at[3]),
             local(w_hbm, wv, in_sem.at[4])]
    for copy in loads[:3]:
        copy.start()
    XR = tokens // LOADS

    def x_load(m):
        rows = pl.ds(pl.multiple_of(m * XR, XR), XR)
        return local(x_hbm.at[rows, :], xv.at[rows, :], x_sem.at[m])

    barrier = pltpu.get_barrier_semaphore()
    for d in range(1, n):
        pl.semaphore_signal(barrier, inc=1, device_id={"sp": lax.rem(me + d, n)}, device_id_type=MESH)
    for d in range(1, ntp):
        pl.semaphore_signal(barrier, inc=1, device_id={"tp": lax.rem(tpi + d, ntp)}, device_id_type=MESH)

    head_row = iota((ROWS, BLK), 0)
    rate = jnp.zeros((ROWS, BLK), F32)
    for h in range(heads):
        rate = jnp.where(head_row == h, jnp.broadcast_to(log_ref[h], (ROWS, BLK)), rate)
    rate = jnp.where(head_row < heads, jnp.exp(rate), 0.0)
    run_s[...] = jnp.zeros_like(run_s)
    for b in range(blocks):
        run_s[b * ROWS:b * ROWS + heads, :] = pre_ref[:, b * BLK:(b + 1) * BLK]
    pre_all = run_s[...]
    step_all = jnp.maximum(pre_all, 0.0) + jnp.log1p(jnp.exp(-jnp.abs(pre_all)))
    step_s[...] = step_all
    lanes = iota((blocks * ROWS, BLK), 1)
    acc = -jnp.concatenate([rate] * blocks, axis=0) * step_all
    shift = 1
    while shift < BLK:
        acc = acc + jnp.where(lanes >= shift, pltpu.roll(acc, shift, 1), 0.0)
        shift *= 2
    run_s[...] = acc
    runs_all = acc - jnp.log(step_all)
    runs_s[...] = runs_all
    for b in range(blocks):
        rows = slice(b * ROWS, (b + 1) * ROWS)
        cols_s[b * BLK:(b + 1) * BLK, :] = jnp.concatenate([acc[rows], runs_all[rows]], axis=0).T

    spread = jnp.where((iota((3 * ROWS, wide), 0) & (ROWS - 1)) == iota((3 * ROWS, wide), 1) // HEAD,
                       1.0, 0.0).astype(BF)
    pick = jnp.where(iota((ROWS, wide), 0) == iota((ROWS, wide), 1) // HEAD, 1.0, 0.0).astype(BF)
    at_row, at_col = iota((BLK, BLK), 0), iota((BLK, BLK), 1)

    def toks(b):
        return pl.ds(pl.multiple_of(b * BLK, BLK), BLK)

    def heads8(b):
        return pl.ds(pl.multiple_of(b * ROWS, ROWS), ROWS)

    def lanes_of(u):
        return slice(u * gw, (u + 1) * gw)

    def placed(a, u):
        rows = [a if g == u else jnp.zeros_like(a) for g in range(groups)]
        return rows[0] if groups == 1 else jnp.concatenate(rows, axis=0)

    def from_start(b, u):
        return dot(thirds(jnp.exp(run_s[heads8(b), :])), spread[:, lanes_of(u)], 0, 0)

    def to_end(b):
        run, runs = run_s[heads8(b), :], runs_s[heads8(b), :]
        return dot(thirds(jnp.exp(run[:, BLK - 1:BLK] - runs)), spread, 0, 0)

    def row_copy(i, d):
        return remote(row_in.at[i, 0], row_in.at[i, d], row_ss.at[i, d - 1], row_rs.at[i, d - 1], "sp",
                      z * X + lax.rem(x + d, X))

    def col_copy(i, d, back):
        to = lax.rem(z + (Z - d if back else d), Z) * X + x
        return remote(col_out.at[i], col_in.at[i, d - 1], col_ss.at[i, d - 1], col_rs.at[i, d - 1], "sp", to)

    def sends_to(d, back):
        return (z >= d) if back else (z + d < Z)

    def hears_from(d, back):
        return (z + d < Z) if back else (z >= d)

    def row_start(i, state, decayed):
        row_in[i, 0, 0:STATE, :] = state
        row_in[i, 0, STATE:STATE + ROWS, :] = decayed
        for d in range(1, X):
            row_copy(i, d).start()

    def row_finish(i, back):
        for d in range(1, X):
            row_copy(i, d).wait_recv()
        acc, fac = jnp.zeros((STATE, gw), F32), jnp.ones((ROWS, gw), F32)
        mine, mine_fac = acc, fac
        for xx in (reversed(range(X)) if back else range(X)):
            mine = jnp.where(x == xx, acc, mine)
            mine_fac = jnp.where(x == xx, fac, mine_fac)
            item = row_in[i, lax.rem(x - xx + X, X)]
            acc = item[0:STATE] + acc * item[STATE:STATE + 1]
            fac = fac * item[STATE:STATE + ROWS]
        pass_s[i, 0:STATE, :] = mine
        pass_s[i, STATE:STATE + ROWS, :] = mine_fac
        col_out[i, 0:STATE, :] = acc
        col_out[i, STATE:STATE + ROWS, :] = fac
        for d in range(1, Z):
            @pl.when(sends_to(d, back))
            def _(d=d):
                col_copy(i, d, back).start()

    def col_finish(i, back, into, u):
        into[u] = pass_s[i, 0:STATE, :]
        for d in range(1, Z):
            @pl.when(hears_from(d, back))
            def _(d=d):
                col_copy(i, d, back).wait_recv()
                into[u] += col_in[i, d - 1, 0:STATE, :] * pass_s[i, STATE:STATE + 1, :]
                pass_s[i, STATE:STATE + ROWS, :] *= col_in[i, d - 1, STATE:STATE + ROWS, :]

    for copy in loads[:3]:
        copy.wait()
    for copy in loads[3:]:
        copy.start()
    for m in range(LOADS):
        x_load(m).start()

    def reverse(u):
        gs = lanes_of(u)
        dstates[u, blocks] = jnp.zeros((STATE, gw), F32)

        def body(i, decayed):
            b = blocks - 1 - i
            tk = toks(b)
            gate, cot = gv[tk, gs].astype(F32), ov[tk, gs].astype(F32)
            sig = sigmoid(gate)
            cs = cot * sig
            grads = cs * gate
            grads_s[tk, gs] = grads
            dgate_s[tk, gs] = cs * (1.0 + gate * (1.0 - sig))
            fs = from_start(b, u)
            gfs = (grads * fs).astype(BF)
            gfs_s[tk, gs] = gfs
            factor = fs[BLK - 1:BLK, :]
            fac_s[b, :, gs] = jnp.broadcast_to(factor, (ROWS, gw))
            after_s[b, :, gs] = decayed
            back = dot(qv[tk, :], gfs, 0, 0)[u * STATE:(u + 1) * STATE]
            dstates[u, b] = dstates[u, b + 1] * factor + back
            return decayed * factor

        return lax.fori_loop(0, blocks, body, jnp.ones((ROWS, gw), F32), unroll=4)

    def inner_grads(u, b):
        gs = lanes_of(u)
        tk = toks(b)
        run = run_s[heads8(b), :]
        key, query = kv[tk, :], qv[tk, :]
        if u == 0:
            te_all = to_end(b)
            te_s[tk, :] = te_all
            te = te_all[:, gs]
        else:
            te = te_s[tk, gs]
        mine = iota((BLK, narrow), 1) // STATE == u
        scores = dot(key, jnp.where(mine, query, jnp.zeros_like(query)), 1, 1)
        cols = cols_s[tk, :]
        outer = dot(key, placed(dstates[u, b + 1].astype(BF), u), 1, 0) * te
        weights = []
        for h in range(u * ratio, (u + 1) * ratio):
            decay = jnp.exp(jnp.where(at_col >= at_row, run[h:h + 1, :] - cols[:, ROWS + h:ROWS + h + 1], -1e30))
            weights.append((scores * decay).astype(BF))
        spread_grads = by_blocks(grads_s[tk, gs].astype(BF), ratio, HEAD)
        dval_s[tk, gs] = dot(jnp.concatenate(weights, axis=1), spread_grads, 1, 0) + outer

    def forward():
        for u in range(groups):
            states[u, 0] = jnp.zeros((STATE, gw), F32)

        def body(b, before):
            tk = toks(b)
            vte = (vals_s[tk, :] * te_s[tk, :]).astype(BF)
            vte_s[tk, :] = vte
            factor = fac_s[b]
            ahead_s[b] = before
            add = dot(kv[tk, :], vte, 0, 0)
            for u in range(groups):
                gs = lanes_of(u)
                states[u, b + 1] = states[u, b] * factor[0:1, gs] + add[u * STATE:(u + 1) * STATE, gs]
            return before * factor

        return lax.fori_loop(0, blocks, body, jnp.ones((ROWS, wide), F32), unroll=4)

    def correct(u):
        gs = lanes_of(u)

        def body(b, carry):
            tk = toks(b)
            extra = (outgo_s[u] * after_s[b, 0:1, gs]).astype(BF)
            dval = dval_s[tk, gs] + dot(kv[tk, :], placed(extra, u), 1, 0) * te_s[tk, gs]
            dval_s[tk, gs] = dval
            vgt_s[gs, tk] = (dval * vslope_s[tk, gs]).T.astype(BF)
            return carry

        lax.fori_loop(0, blocks, body, 0, unroll=4)

    def chunk_of(k):
        out = jnp.int32(0)
        for i in range(Z):
            order = sorted(range(Z), key=lambda zc: -abs(zc - i))
            here = jnp.int32(0)
            for kk in range(Z):
                here = jnp.where(k == kk, order[kk], here)
            out = jnp.where(z == i, here, out)
        return out

    def piece_rows(q):
        return pl.ds(pl.multiple_of(q * PIECE, PIECE), PIECE)

    def x_copy(t, q):
        to = z * X + lax.rem(x + 1 + t // Z, X)
        return remote(part.at[t, piece_rows(q), :], xrecv.at[t, piece_rows(q), :], xs.at[t * NP + q],
                      xr.at[t * NP + q], "sp", to)

    def z_next(zc):
        to = jnp.where(zc < z, z - 1, z + 1)
        slot = jnp.where((zc > z) & (zc == to), Z, zc)
        return lax.rem(to * X + x + n, n), slot

    def z_copy(k, q):
        to, slot = z_next(chunk_of(k))
        return remote(part.at[(X - 1) * Z + k, piece_rows(q), :], zbuf.at[slot, piece_rows(q), :],
                      zs.at[k * NP + q], zr.at[slot * NP + q], "sp", to)

    def z_arrival(slot, q):
        return remote(part.at[0, piece_rows(q), :], zbuf.at[slot, piece_rows(q), :], zs.at[q],
                      zr.at[slot * NP + q], "sp", lax.rem(me + X, n))

    def zl_copy(t):
        to, slot = z_next(chunk_of(lax.rem(t, Z)))
        at = (t // Z) * (Z + 1) + slot
        return remote(part.at[t, 0:PIECE, :], zlast.at[at], zls.at[t], zlr.at[at], "sp", to)

    def zl_arrival(at):
        return remote(part.at[0, 0:PIECE, :], zlast.at[at], zls.at[0], zlr.at[at], "sp", lax.rem(me + X, n))

    def xl_copy(xi):
        k = Z - 1
        return remote(part.at[xi * Z + k, 0:PIECE, :], xlast.at[xi], xls.at[xi], xlr.at[xi], "sp",
                      z * X + lax.rem(x + 1 + xi, X))

    def upstream(zc):
        return ((zc <= z) & (z < Z - 1)) | ((zc > z) & (z > 0))

    def chunks(u, low, high, beside):
        def body(t, carry):
            beside(t)
            k = lax.rem(t, Z)
            zc = chunk_of(k)
            dest = zc * X + lax.rem(x + 1 + t // Z, X)
            step = min(256, CD)
            for half in range(CD // step):
                cs = pl.ds(pl.multiple_of(dest * CD + half * step, 128), step)
                part[t, lanes_of(u), half * step:(half + 1) * step] = jnp.dot(
                    vgt_s[lanes_of(u), :], xv[:, cs], preferred_element_type=F32)

            @pl.when(t < (X - 1) * Z)
            def _():
                for q in range(u * PU, (u + 1) * PU):
                    if q > 0:
                        x_copy(t, q).start()

            if u == 0:
                @pl.when((zc != z) & jnp.logical_not(upstream(zc)))
                def _():
                    zl_copy(t).start()
            return carry

        lax.fori_loop(low, high, body, 0)

    def last_rows(i, carry):
        k = i // X
        xi = lax.rem(i, X)
        t = xi * Z + k
        zc = chunk_of(k)
        base = xi * (Z + 1)

        @pl.when(upstream(zc))
        def _():
            zl_arrival(base + zc).wait_recv()
            part[t, 0:PIECE, :] += zlast[base + zc]

        @pl.when((zc == z) & (z > 0))
        def _():
            zl_arrival(base + Z).wait_recv()
            part[t, 0:PIECE, :] += zlast[base + Z]

        @pl.when((zc != z) & upstream(zc))
        def _():
            zl_copy(t).start()

        @pl.when((zc == z) & (xi < X - 1))
        def _():
            xl_copy(xi).start()
        return carry

    def grads_of(b):
        tk = toks(b)
        key, query = kv[tk, :], qv[tk, :]
        grads, vals = grads_s[tk, :], vals_s[tk, :]
        grads_b, vals_b = grads.astype(BF), vals.astype(BF)
        run, runs = run_s[heads8(b), :], runs_s[heads8(b), :]
        cols = cols_s[tk, :]
        state, dstate, cross_lanes = [], [], []
        for u in range(groups):
            gs = lanes_of(u)
            before, factor = ahead_s[b, 0:1, gs], fac_s[b, 0:1, gs]
            state.append(placed((states[u, b] + before * income_s[u]).astype(BF), u))
            after = states[u, b + 1] + (before * factor) * income_s[u]
            down = dstates[u, b + 1] + after_s[b, 0:1, gs] * outgo_s[u]
            dstate.append(placed(down.astype(BF), u))
            cross_lanes.append(jnp.sum(after * down, axis=0, keepdims=True))
        join = (lambda v: v[0]) if groups == 1 else (lambda v: jnp.concatenate(v, axis=1))
        state_b, dstate_b = join(state), join(dstate)
        keys = by_blocks(key, groups, STATE)
        scores = dot(query, keys, 1, 1)
        pulled = dot(grads_b, by_blocks(vals_b, heads, HEAD), 1, 1)
        fs = dot(thirds(jnp.exp(run)), spread, 0, 0)
        outer = dot(query, state_b, 1, 0) * fs
        totals = []
        mixed = []
        for g in range(groups):
            weights, total = [], None
            for h in range(g * ratio, (g + 1) * ratio):
                decay = jnp.exp(jnp.where(at_row >= at_col, cols[:, h:h + 1] - runs[h:h + 1, :], -1e30))
                weights.append((scores[:, g * BLK:(g + 1) * BLK] * decay).astype(BF))
                item = pulled[:, h * BLK:(h + 1) * BLK] * decay
                total = item if total is None else total + item
            totals.append(total.astype(BF))
            gs = lanes_of(g)
            inner = dot(jnp.concatenate(weights, axis=1), by_blocks(vals_b[:, gs], ratio, HEAD), 1, 0)
            mixed.append(inner + outer[:, gs])
        mixed = join(mixed)
        dgate_s[tk, :] = mixed * dgate_s[tk, :]
        total = join(totals)
        dquery_s[tk, :] = dot(gfs_s[tk, :], state_b, 1, 1) + dot(total, keys, 1, 0)
        across = dot(total, query, 0, 0)
        dkey = dot(vte_s[tk, :], dstate_b, 1, 1)
        mine = across[0:BLK]
        for g in range(1, groups):
            mine = jnp.where(iota((BLK, narrow), 1) // STATE == g, across[g * BLK:(g + 1) * BLK], mine)
        dkey_s[tk, :] = dkey + mine
        there = sum(dot(pick, part_, 1, 1) for part_ in halves(grads * mixed))
        here = sum(dot(pick, part_, 1, 1) for part_ in halves(vals * dval_s[tk, :]))
        cross = jnp.sum(jnp.where(iota((ROWS, wide), 0) == iota((ROWS, wide), 1) // HEAD, join(cross_lanes), 0.0),
                        axis=1, keepdims=True)
        back = there - here
        lane = iota((ROWS, BLK), 1)
        shift = 1
        while shift < BLK:
            back = back + jnp.where(lane < BLK - shift, pltpu.roll(back, BLK - shift, 1), 0.0)
            shift *= 2
        pre = pre_ref[:, tk]
        size_total = (here / step_s[heads8(b), :] - rate * (back + cross))[0:heads]
        ddecay_ref[:, tk] = size_total * sigmoid(pre)

    pass0, pass1 = (Z - 1) * (PU - 1), (Z - 1) * PU * (groups - 1)

    def reduce(s):
        less = max(1, PU - 1)
        r = jnp.clip(s - pass0, 0, max(0, pass1 - 1))
        k = jnp.where(s < pass0, s // less, lax.rem(r // PU, max(1, Z - 1)))
        q = jnp.where(s < pass0, 1 + lax.rem(s, less), (1 + r // (PU * max(1, Z - 1))) * PU + lax.rem(r, PU))
        k = jnp.where(s < pass0 + pass1, k, Z - 1)
        q = jnp.where(s < pass0 + pass1, q, 1 + jnp.maximum(s - pass0 - pass1, 0))
        zc = chunk_of(k)
        rows = piece_rows(q)
        mine = (X - 1) * Z + k
        total = part[mine, rows, :]
        for xi in range(X - 1):
            x_copy(xi * Z + k, q).wait_recv()
            total = total + xrecv[xi * Z + k, rows, :]
        part[mine, rows, :] = total

        @pl.when(upstream(zc))
        def _():
            z_arrival(zc, q).wait_recv()
            part[mine, rows, :] += zbuf[zc, rows, :]

        @pl.when((zc == z) & (z > 0))
        def _():
            z_arrival(Z, q).wait_recv()
            part[mine, rows, :] += zbuf[Z, rows, :]

        @pl.when(zc != z)
        def _():
            z_copy(k, q).start()

    REV, FWD = 0, groups
    for u in range(groups):
        decayed = reverse(u)
        if u == 0:
            pl.semaphore_wait(barrier, n - 1 + ntp - 1)
        row_start(REV + u, dstates[u, 0], decayed)
    row_finish(REV, True)
    for copy in loads[3:]:
        copy.wait()
    per = blocks // LOADS

    def project(m, carry):
        x_load(m).wait()
        rows = pl.ds(pl.multiple_of(m * XR, XR), XR)
        pre = jnp.dot(xv[rows, :], wv[...], preferred_element_type=F32).astype(BF).astype(F32)
        sig = sigmoid(pre)
        vals_s[rows, :] = pre * sig
        vslope_s[rows, :] = sig * (1.0 + pre * (1.0 - sig))
        for i in range(per):
            inner_grads(0, m * per + i)
        return carry

    half = LOADS // 2
    lax.fori_loop(0, half, project, 0)
    for u in range(1, groups):
        row_finish(REV + u, True)
    lax.fori_loop(half, LOADS, project, 0)
    decayed = forward()
    for u in range(groups):
        row_start(FWD + u, states[u, blocks], decayed[:, lanes_of(u)])
    col_finish(REV, True, outgo_s, 0)
    correct(0)
    steps = Z * (NP - 1)
    early = min(2 * (Z - 1), X * Z, (Z - 1) * (PU - 1)) if groups > 1 else 0
    at_end = (z == 0) | (z == Z - 1)

    def quiet(t):
        pass

    def early_step(t):
        @pl.when(at_end & (t < early))
        def _():
            reduce(t)

    chunks(0, 0, Z, quiet)
    for u in range(groups):
        row_finish(FWD + u, False)
    chunks(0, Z, X * Z, quiet)
    for u in range(1, groups):
        def inner(b, carry, u=u):
            inner_grads(u, b)
            return carry

        lax.fori_loop(0, blocks, inner, 0, unroll=4)
        col_finish(REV + u, True, outgo_s, u)
        correct(u)
        chunks(u, 0, X * Z, early_step if u == 1 else quiet)

    def alone(s, carry):
        @pl.when(jnp.logical_not(at_end & (s < early)))
        def _():
            reduce(s)
        return carry

    near = (Z - 1) * X
    lax.fori_loop(0, near, last_rows, 0)
    lax.fori_loop(0, early, alone, 0)
    for u in range(groups):
        col_finish(FWD + u, False, income_s, u)

    def both(i, carry):
        for r in range(2):
            @pl.when(early + 2 * i + r < steps)
            def _(r=r):
                reduce(early + 2 * i + r)

        @pl.when(i == blocks // 4)
        def _():
            lax.fori_loop(near, Z * X, last_rows, 0)

        for r in range(2):
            grads_of(2 * i + r)
        return carry

    lax.fori_loop(0, blocks // 2, both, 0)
    outs = [local(dkey_s, dkey_hbm, o_sem.at[0]), local(dquery_s, dquery_hbm, o_sem.at[1]),
            local(dgate_s, dgate_hbm, o_sem.at[2])]
    for copy in outs:
        copy.start()
    if early + blocks < steps:
        lax.fori_loop(early + blocks, steps, alone, 0)

    own = X * Z - 1
    for xi in range(X - 1):
        xl_copy(xi).wait_recv()
        part[own, 0:PIECE, :] += xlast[xi]
    last = part[own]
    norms[tpi] = jnp.broadcast_to(jnp.sum(last * last, axis=0, keepdims=True), (ROWS, CD))

    def norm_copy(d):
        return remote(norms.at[tpi], norms.at[tpi], ns.at[d - 1], nr.at[d - 1], "tp", lax.rem(tpi + d, ntp))

    for d in range(1, ntp):
        norm_copy(d).start()
    wg_s[...] = last.T
    wcopy = local(wg_s, wgrad_hbm, o_sem.at[3])
    wcopy.start()

    for i in range(2 * groups):
        back = i < groups
        for d in range(1, X):
            row_copy(i, d).wait_send()
        for d in range(1, Z):
            @pl.when(sends_to(d, back))
            def _(i=i, d=d, back=back):
                col_copy(i, d, back).wait_send()

    def sent(t, carry):
        x_copy(t // (NP - 1), 1 + lax.rem(t, NP - 1)).wait_send()
        return carry

    def passed(t, carry):
        z_copy(t // (NP - 1), 1 + lax.rem(t, NP - 1)).wait_send()
        return carry

    def passed_last(i, carry):
        zl_copy((i // (Z - 1)) * Z + lax.rem(i, Z - 1)).wait_send()
        return carry

    lax.fori_loop(0, (X - 1) * Z * (NP - 1), sent, 0)
    lax.fori_loop(0, (Z - 1) * (NP - 1), passed, 0)
    lax.fori_loop(0, X * (Z - 1), passed_last, 0)
    for xi in range(X - 1):
        xl_copy(xi).wait_send()
    for d in range(1, ntp):
        got = remote(norms.at[tpi], norms.at[lax.rem(tpi + ntp - d, ntp)], ns.at[d - 1], nr.at[d - 1], "tp",
                     lax.rem(tpi + d, ntp))
        got.wait()
    total = norms[0]
    for i in range(1, ntp):
        total = total + norms[i]
    norm_ref[...] = total[0:1]
    for copy in outs:
        copy.wait()
    wcopy.wait()


def shards(block_input, value_weight, key_rows, query_rows, decay_pre, decay_log, gate_rows, out_grad):
    heads = decay_log.shape[0]
    tokens, depth = block_input.shape
    groups = key_rows.shape[1] // STATE
    wide, narrow = heads * HEAD, groups * STATE
    blocks = tokens // BLK
    n, ntp = lax.axis_size("sp"), lax.axis_size("tp")
    X = max(1, ntp // 2)
    if n % X:
        X = 1
    Z = n // X
    cd = depth // n
    gw = heads // groups * HEAD
    NP = wide // PIECE
    XO = max(1, X - 1)
    c = dict(heads=heads, ratio=heads // groups, blocks=blocks, n=n, ntp=ntp, X=X, Z=Z, cd=cd)
    hbm = pl.BlockSpec(memory_space=pl.ANY)
    vmem = pl.BlockSpec(memory_space=pltpu.VMEM)
    V = pltpu.VMEM
    dma = pltpu.SemaphoreType.DMA
    outs = pl.pallas_call(
        functools.partial(kernel, c),
        in_specs=[hbm, hbm, hbm, hbm, vmem, pl.BlockSpec(memory_space=pltpu.SMEM), hbm, hbm],
        out_specs=[hbm, hbm, vmem, hbm, hbm, vmem],
        out_shape=[
            jax.ShapeDtypeStruct((tokens, narrow), F32),
            jax.ShapeDtypeStruct((tokens, narrow), F32),
            jax.ShapeDtypeStruct((heads, tokens), F32),
            jax.ShapeDtypeStruct((tokens, wide), F32),
            jax.ShapeDtypeStruct((cd, wide), F32),
            jax.ShapeDtypeStruct((1, cd), F32),
        ],
        scratch_shapes=[
            V((tokens, depth), BF), V((depth, wide), BF), V((tokens, narrow), BF), V((tokens, narrow), BF),
            V((tokens, wide), BF), V((tokens, wide), BF),
            V((blocks * ROWS, BLK), F32), V((blocks * ROWS, BLK), F32), V((blocks * ROWS, BLK), F32),
            V((tokens, 2 * ROWS), F32), V((tokens, wide), F32), V((tokens, wide), BF),
            V((groups, blocks + 1, STATE, gw), F32), V((groups, blocks + 1, STATE, gw), F32),
            V((blocks, ROWS, wide), F32), V((blocks, ROWS, wide), F32), V((blocks, ROWS, wide), F32),
            V((tokens, wide), F32), V((tokens, wide), F32), V((tokens, wide), F32), V((tokens, wide), F32),
            V((tokens, wide), BF), V((tokens, wide), F32), V((tokens, narrow), F32), V((tokens, narrow), F32),
            V((wide, tokens), BF), V((X * Z, wide, cd), F32), V((XO * Z, wide, cd), F32),
            V((Z + 1, wide, cd), F32), V((X * (Z + 1), PIECE, cd), F32), V((XO, PIECE, cd), F32),
            V((2 * groups, X, STATE + ROWS, gw), F32), V((2 * groups, STATE + ROWS, gw), F32),
            V((2 * groups, Z - 1, STATE + ROWS, gw), F32),
            V((groups, STATE, gw), F32), V((groups, STATE, gw), F32), V((2 * groups, STATE + ROWS, gw), F32),
            V((cd, wide), F32), V((ntp, ROWS, cd), F32),
            dma((5,)), dma((LOADS,)),
            dma((2 * groups, XO)), dma((2 * groups, XO)), dma((2 * groups, Z - 1)), dma((2 * groups, Z - 1)),
            dma((XO * Z * NP,)), dma((XO * Z * NP,)), dma((Z * NP,)), dma(((Z + 1) * NP,)),
            dma((X * Z,)), dma((X * (Z + 1),)), dma((XO,)), dma((XO,)),
            dma((ntp - 1,)), dma((ntp - 1,)), dma((4,)),
        ],
        compiler_params=pltpu.CompilerParams(
            collective_id=0, has_side_effects=True, vmem_limit_bytes=66_000_000),
        name="mixer_back",
    )(block_input, value_weight, key_rows, query_rows, decay_pre, decay_log, gate_rows, out_grad)
    key_grad, query_grad, decay_grad, gate_grad, weight_grad, norm = outs
    return key_grad, query_grad, decay_grad, gate_grad, weight_grad, norm.reshape(cd)


def solution(mesh):
    in_specs = (
        P("sp", None),
        P(None, "tp"),
        P("sp", "tp"),
        P("sp", "tp"),
        P("tp", "sp"),
        P("tp"),
        P("sp", "tp"),
        P("sp", "tp"),
    )
    out_specs = (P("sp", "tp"), P("sp", "tp"), P("tp", "sp"), P("sp", "tp"), P("sp", "tp"), P("sp"))
    return jax.shard_map(shards, mesh=mesh, in_specs=in_specs, out_specs=out_specs, check_vma=False)
```

```python
import functools

import jax
import jax.numpy as jnp
from jax import lax
from jax.experimental import pallas as pl
from jax.experimental.pallas import tpu as pltpu
from jax.sharding import PartitionSpec as P

HEAD = 64
STATE = 64
BLK = 128
ROWS = 8
LOADS = 8
PIECE = 32

BF = jnp.bfloat16
F32 = jnp.float32
MESH = pl.DeviceIdType.MESH


def dot(a, b, ca, cb):
    return lax.dot_general(a, b, (((ca,), (cb,)), ((), ())), preferred_element_type=F32)


def iota(shape, dim):
    return lax.broadcasted_iota(jnp.int32, shape, dim)


def sigmoid(v):
    return 1.0 / (1.0 + jnp.exp(-v))


def thirds(q):
    hi = q.astype(BF).astype(F32)
    rest = q - hi
    mid = rest.astype(BF).astype(F32)
    return jnp.concatenate([hi, mid, rest - mid], axis=0).astype(BF)


def halves(q):
    hi = q.astype(BF)
    return hi, (q - hi.astype(F32)).astype(BF)


def by_blocks(a, count, width):
    if count == 1:
        return a
    lane = iota(a.shape, 1) // width
    return jnp.concatenate([jnp.where(lane == i, a, jnp.zeros_like(a)) for i in range(count)], axis=0)


def kernel(c, x_hbm, w_hbm, key_hbm, query_hbm, pre_ref, log_ref, gate_hbm, out_hbm,
           dkey_hbm, dquery_hbm, ddecay_hbm, dgate_hbm, wgrad_hbm, norm_hbm,
           xv, wv, kv, qv, gv, ov, run_s, runs_s, step_s, cols_s, grads_s, gfs_s, dstates, states,
           fac_s, after_s, ahead_s, vals_s, te_s, dval_s, vslope_s, vte_s, dgate_s, dkey_s, dquery_s,
           vgt_s, part, xrecv, zbuf, zlast, xlast, row_in, col_out, col_in, outgo_s, income_s, pass_s,
           wg_s, norms, ddecay_s, norm_s,
           in_sem, x_sem, row_ss, row_rs, col_ss, col_rs, xs, xr, zs, zr, zls, zlr, xls, xlr, ns, nr, o_sem):
    heads, ratio, blocks, n, ntp, X, Z = c["heads"], c["ratio"], c["blocks"], c["n"], c["ntp"], c["X"], c["Z"]
    groups = heads // ratio
    wide, narrow, CD = heads * HEAD, groups * STATE, c["cd"]
    gw = ratio * HEAD
    PU = gw // PIECE
    NP = groups * PU
    tokens = blocks * BLK
    me, tpi = lax.axis_index("sp"), lax.axis_index("tp")
    z, x = me // X, lax.rem(me, X)

    def local(src, dst, sem):
        return pltpu.make_async_copy(src, dst, sem)

    def remote(src, dst, ssem, rsem, axis, to):
        return pltpu.make_async_remote_copy(src, dst, ssem, rsem, device_id={axis: to}, device_id_type=MESH)

    loads = [local(gate_hbm, gv, in_sem.at[0]), local(out_hbm, ov, in_sem.at[1]),
             local(query_hbm, qv, in_sem.at[2]), local(key_hbm, kv, in_sem.at[3]),
             local(w_hbm, wv, in_sem.at[4])]
    for copy in loads[:3]:
        copy.start()
    XR = tokens // LOADS

    def x_load(m):
        rows = pl.ds(pl.multiple_of(m * XR, XR), XR)
        return local(x_hbm.at[rows, :], xv.at[rows, :], x_sem.at[m])

    barrier = pltpu.get_barrier_semaphore()
    for d in range(1, n):
        pl.semaphore_signal(barrier, inc=1, device_id={"sp": lax.rem(me + d, n)}, device_id_type=MESH)
    for d in range(1, ntp):
        pl.semaphore_signal(barrier, inc=1, device_id={"tp": lax.rem(tpi + d, ntp)}, device_id_type=MESH)

    head_row = iota((ROWS, BLK), 0)
    rate = jnp.zeros((ROWS, BLK), F32)
    for h in range(heads):
        rate = jnp.where(head_row == h, jnp.broadcast_to(log_ref[h], (ROWS, BLK)), rate)
    rate = jnp.where(head_row < heads, jnp.exp(rate), 0.0)
    run_s[...] = jnp.zeros_like(run_s)
    for b in range(blocks):
        run_s[b * ROWS:b * ROWS + heads, :] = pre_ref[:, b * BLK:(b + 1) * BLK]
    pre_all = run_s[...]
    step_all = jnp.maximum(pre_all, 0.0) + jnp.log1p(jnp.exp(-jnp.abs(pre_all)))
    step_s[...] = step_all
    lanes = iota((blocks * ROWS, BLK), 1)
    acc = -jnp.concatenate([rate] * blocks, axis=0) * step_all
    shift = 1
    while shift < BLK:
        acc = acc + jnp.where(lanes >= shift, pltpu.roll(acc, shift, 1), 0.0)
        shift *= 2
    run_s[...] = acc
    runs_all = acc - jnp.log(step_all)
    runs_s[...] = runs_all
    for b in range(blocks):
        rows = slice(b * ROWS, (b + 1) * ROWS)
        cols_s[b * BLK:(b + 1) * BLK, :] = jnp.concatenate([acc[rows], runs_all[rows]], axis=0).T

    spread = jnp.where((iota((3 * ROWS, wide), 0) & (ROWS - 1)) == iota((3 * ROWS, wide), 1) // HEAD,
                       1.0, 0.0).astype(BF)
    pick = jnp.where(iota((ROWS, wide), 0) == iota((ROWS, wide), 1) // HEAD, 1.0, 0.0).astype(BF)
    at_row, at_col = iota((BLK, BLK), 0), iota((BLK, BLK), 1)

    def toks(b):
        return pl.ds(pl.multiple_of(b * BLK, BLK), BLK)

    def heads8(b):
        return pl.ds(pl.multiple_of(b * ROWS, ROWS), ROWS)

    def lanes_of(u):
        return slice(u * gw, (u + 1) * gw)

    def placed(a, u):
        rows = [a if g == u else jnp.zeros_like(a) for g in range(groups)]
        return rows[0] if groups == 1 else jnp.concatenate(rows, axis=0)

    def from_start(b, u):
        return dot(thirds(jnp.exp(run_s[heads8(b), :])), spread[:, lanes_of(u)], 0, 0)

    def to_end(b):
        run, runs = run_s[heads8(b), :], runs_s[heads8(b), :]
        return dot(thirds(jnp.exp(run[:, BLK - 1:BLK] - runs)), spread, 0, 0)

    def row_copy(i, d):
        return remote(row_in.at[i, 0], row_in.at[i, d], row_ss.at[i, d - 1], row_rs.at[i, d - 1], "sp",
                      z * X + lax.rem(x + d, X))

    def col_copy(i, d, back):
        to = lax.rem(z + (Z - d if back else d), Z) * X + x
        return remote(col_out.at[i], col_in.at[i, d - 1], col_ss.at[i, d - 1], col_rs.at[i, d - 1], "sp", to)

    def sends_to(d, back):
        return (z >= d) if back else (z + d < Z)

    def hears_from(d, back):
        return (z + d < Z) if back else (z >= d)

    def row_start(i, state, decayed):
        row_in[i, 0, 0:STATE, :] = state
        row_in[i, 0, STATE:STATE + ROWS, :] = decayed
        for d in range(1, X):
            row_copy(i, d).start()

    def row_finish(i, back):
        for d in range(1, X):
            row_copy(i, d).wait_recv()
        acc, fac = jnp.zeros((STATE, gw), F32), jnp.ones((ROWS, gw), F32)
        mine, mine_fac = acc, fac
        for xx in (reversed(range(X)) if back else range(X)):
            mine = jnp.where(x == xx, acc, mine)
            mine_fac = jnp.where(x == xx, fac, mine_fac)
            item = row_in[i, lax.rem(x - xx + X, X)]
            acc = item[0:STATE] + acc * item[STATE:STATE + 1]
            fac = fac * item[STATE:STATE + ROWS]
        pass_s[i, 0:STATE, :] = mine
        pass_s[i, STATE:STATE + ROWS, :] = mine_fac
        col_out[i, 0:STATE, :] = acc
        col_out[i, STATE:STATE + ROWS, :] = fac
        for d in range(1, Z):
            @pl.when(sends_to(d, back))
            def _(d=d):
                col_copy(i, d, back).start()

    def col_finish(i, back, into, u):
        into[u] = pass_s[i, 0:STATE, :]
        for d in range(1, Z):
            @pl.when(hears_from(d, back))
            def _(d=d):
                col_copy(i, d, back).wait_recv()
                into[u] += col_in[i, d - 1, 0:STATE, :] * pass_s[i, STATE:STATE + 1, :]
                pass_s[i, STATE:STATE + ROWS, :] *= col_in[i, d - 1, STATE:STATE + ROWS, :]

    for copy in loads[:3]:
        copy.wait()
    for copy in loads[3:]:
        copy.start()

    def reverse(u):
        gs = lanes_of(u)
        dstates[u, blocks] = jnp.zeros((STATE, gw), F32)

        def body(i, decayed):
            b = blocks - 1 - i
            tk = toks(b)
            gate, cot = gv[tk, gs].astype(F32), ov[tk, gs].astype(F32)
            sig = sigmoid(gate)
            cs = cot * sig
            grads = cs * gate
            grads_s[tk, gs] = grads
            dgate_s[tk, gs] = cs * (1.0 + gate * (1.0 - sig))
            fs = from_start(b, u)
            gfs = (grads * fs).astype(BF)
            gfs_s[tk, gs] = gfs
            factor = fs[BLK - 1:BLK, :]
            fac_s[b, :, gs] = jnp.broadcast_to(factor, (ROWS, gw))
            after_s[b, :, gs] = decayed
            back = dot(qv[tk, :], gfs, 0, 0)[u * STATE:(u + 1) * STATE]
            dstates[u, b] = dstates[u, b + 1] * factor + back
            return decayed * factor

        return lax.fori_loop(0, blocks, body, jnp.ones((ROWS, gw), F32), unroll=4)

    def inner_grads(u, b):
        gs = lanes_of(u)
        tk = toks(b)
        run = run_s[heads8(b), :]
        key, query = kv[tk, :], qv[tk, :]
        if u == 0:
            te_all = to_end(b)
            te_s[tk, :] = te_all
            te = te_all[:, gs]
        else:
            te = te_s[tk, gs]
        mine = iota((BLK, narrow), 1) // STATE == u
        scores = dot(key, jnp.where(mine, query, jnp.zeros_like(query)), 1, 1)
        cols = cols_s[tk, :]
        outer = dot(key, placed(dstates[u, b + 1].astype(BF), u), 1, 0) * te
        weights = []
        for h in range(u * ratio, (u + 1) * ratio):
            decay = jnp.exp(jnp.where(at_col >= at_row, run[h:h + 1, :] - cols[:, ROWS + h:ROWS + h + 1], -1e30))
            weights.append((scores * decay).astype(BF))
        spread_grads = by_blocks(grads_s[tk, gs].astype(BF), ratio, HEAD)
        dval_s[tk, gs] = dot(jnp.concatenate(weights, axis=1), spread_grads, 1, 0) + outer

    def forward():
        for u in range(groups):
            states[u, 0] = jnp.zeros((STATE, gw), F32)

        def body(b, before):
            tk = toks(b)
            vte = (vals_s[tk, :] * te_s[tk, :]).astype(BF)
            vte_s[tk, :] = vte
            factor = fac_s[b]
            ahead_s[b] = before
            add = dot(kv[tk, :], vte, 0, 0)
            for u in range(groups):
                gs = lanes_of(u)
                states[u, b + 1] = states[u, b] * factor[0:1, gs] + add[u * STATE:(u + 1) * STATE, gs]
            return before * factor

        return lax.fori_loop(0, blocks, body, jnp.ones((ROWS, wide), F32), unroll=4)

    def correct(u):
        gs = lanes_of(u)

        def body(b, carry):
            tk = toks(b)
            extra = (outgo_s[u] * after_s[b, 0:1, gs]).astype(BF)
            dval = dval_s[tk, gs] + dot(kv[tk, :], placed(extra, u), 1, 0) * te_s[tk, gs]
            dval_s[tk, gs] = dval
            vgt_s[gs, tk] = (dval * vslope_s[tk, gs]).T.astype(BF)
            return carry

        lax.fori_loop(0, blocks, body, 0, unroll=4)

    def chunk_of(k):
        out = jnp.int32(0)
        for i in range(Z):
            order = sorted(range(Z), key=lambda zc: -abs(zc - i))
            here = jnp.int32(0)
            for kk in range(Z):
                here = jnp.where(k == kk, order[kk], here)
            out = jnp.where(z == i, here, out)
        return out

    def piece_rows(q):
        return pl.ds(pl.multiple_of(q * PIECE, PIECE), PIECE)

    def x_copy(t, q):
        to = z * X + lax.rem(x + 1 + t // Z, X)
        return remote(part.at[t, piece_rows(q), :], xrecv.at[t, piece_rows(q), :], xs.at[t * NP + q],
                      xr.at[t * NP + q], "sp", to)

    def z_next(zc):
        to = jnp.where(zc < z, z - 1, z + 1)
        slot = jnp.where((zc > z) & (zc == to), Z, zc)
        return lax.rem(to * X + x + n, n), slot

    def z_copy(k, q):
        to, slot = z_next(chunk_of(k))
        return remote(part.at[(X - 1) * Z + k, piece_rows(q), :], zbuf.at[slot, piece_rows(q), :],
                      zs.at[k * NP + q], zr.at[slot * NP + q], "sp", to)

    def z_arrival(slot, q):
        return remote(part.at[0, piece_rows(q), :], zbuf.at[slot, piece_rows(q), :], zs.at[q],
                      zr.at[slot * NP + q], "sp", lax.rem(me + X, n))

    def zl_copy(t):
        to, slot = z_next(chunk_of(lax.rem(t, Z)))
        at = (t // Z) * (Z + 1) + slot
        return remote(part.at[t, 0:PIECE, :], zlast.at[at], zls.at[t], zlr.at[at], "sp", to)

    def zl_arrival(at):
        return remote(part.at[0, 0:PIECE, :], zlast.at[at], zls.at[0], zlr.at[at], "sp", lax.rem(me + X, n))

    def xl_copy(xi):
        k = Z - 1
        return remote(part.at[xi * Z + k, 0:PIECE, :], xlast.at[xi], xls.at[xi], xlr.at[xi], "sp",
                      z * X + lax.rem(x + 1 + xi, X))

    def upstream(zc):
        return ((zc <= z) & (z < Z - 1)) | ((zc > z) & (z > 0))

    def chunks(u, low, high, beside):
        def body(t, carry):
            beside(t)
            k = lax.rem(t, Z)
            zc = chunk_of(k)
            dest = zc * X + lax.rem(x + 1 + t // Z, X)
            step = min(256, CD)
            for half in range(CD // step):
                cs = pl.ds(pl.multiple_of(dest * CD + half * step, 128), step)
                part[t, lanes_of(u), half * step:(half + 1) * step] = jnp.dot(
                    vgt_s[lanes_of(u), :], xv[:, cs], preferred_element_type=F32)

            @pl.when(t < (X - 1) * Z)
            def _():
                for q in range(u * PU, (u + 1) * PU):
                    if q > 0:
                        x_copy(t, q).start()

            if u == 0:
                @pl.when((zc != z) & jnp.logical_not(upstream(zc)))
                def _():
                    zl_copy(t).start()
            return carry

        lax.fori_loop(low, high, body, 0)

    def last_rows(i, carry):
        k = i // X
        xi = lax.rem(i, X)
        t = xi * Z + k
        zc = chunk_of(k)
        base = xi * (Z + 1)

        @pl.when(upstream(zc))
        def _():
            zl_arrival(base + zc).wait_recv()
            part[t, 0:PIECE, :] += zlast[base + zc]

        @pl.when((zc == z) & (z > 0))
        def _():
            zl_arrival(base + Z).wait_recv()
            part[t, 0:PIECE, :] += zlast[base + Z]

        @pl.when((zc != z) & upstream(zc))
        def _():
            zl_copy(t).start()

        @pl.when((zc == z) & (xi < X - 1))
        def _():
            xl_copy(xi).start()
        return carry

    def grads_of(b):
        tk = toks(b)
        key, query = kv[tk, :], qv[tk, :]
        grads, vals = grads_s[tk, :], vals_s[tk, :]
        grads_b, vals_b = grads.astype(BF), vals.astype(BF)
        run, runs = run_s[heads8(b), :], runs_s[heads8(b), :]
        cols = cols_s[tk, :]
        state, dstate, cross_lanes = [], [], []
        for u in range(groups):
            gs = lanes_of(u)
            before, factor = ahead_s[b, 0:1, gs], fac_s[b, 0:1, gs]
            state.append(placed((states[u, b] + before * income_s[u]).astype(BF), u))
            after = states[u, b + 1] + (before * factor) * income_s[u]
            down = dstates[u, b + 1] + after_s[b, 0:1, gs] * outgo_s[u]
            dstate.append(placed(down.astype(BF), u))
            cross_lanes.append(jnp.sum(after * down, axis=0, keepdims=True))
        join = (lambda v: v[0]) if groups == 1 else (lambda v: jnp.concatenate(v, axis=1))
        state_b, dstate_b = join(state), join(dstate)
        keys = by_blocks(key, groups, STATE)
        scores = dot(query, keys, 1, 1)
        pulled = dot(grads_b, by_blocks(vals_b, heads, HEAD), 1, 1)
        fs = dot(thirds(jnp.exp(run)), spread, 0, 0)
        outer = dot(query, state_b, 1, 0) * fs
        totals = []
        mixed = []
        for g in range(groups):
            weights, total = [], None
            for h in range(g * ratio, (g + 1) * ratio):
                decay = jnp.exp(jnp.where(at_row >= at_col, cols[:, h:h + 1] - runs[h:h + 1, :], -1e30))
                weights.append((scores[:, g * BLK:(g + 1) * BLK] * decay).astype(BF))
                item = pulled[:, h * BLK:(h + 1) * BLK] * decay
                total = item if total is None else total + item
            totals.append(total.astype(BF))
            gs = lanes_of(g)
            inner = dot(jnp.concatenate(weights, axis=1), by_blocks(vals_b[:, gs], ratio, HEAD), 1, 0)
            mixed.append(inner + outer[:, gs])
        mixed = join(mixed)
        dgate_s[tk, :] = mixed * dgate_s[tk, :]
        total = join(totals)
        dquery_s[tk, :] = dot(gfs_s[tk, :], state_b, 1, 1) + dot(total, keys, 1, 0)
        across = dot(total, query, 0, 0)
        dkey = dot(vte_s[tk, :], dstate_b, 1, 1)
        mine = across[0:BLK]
        for g in range(1, groups):
            mine = jnp.where(iota((BLK, narrow), 1) // STATE == g, across[g * BLK:(g + 1) * BLK], mine)
        dkey_s[tk, :] = dkey + mine
        there = sum(dot(pick, part_, 1, 1) for part_ in halves(grads * mixed))
        here = sum(dot(pick, part_, 1, 1) for part_ in halves(vals * dval_s[tk, :]))
        cross = jnp.sum(jnp.where(iota((ROWS, wide), 0) == iota((ROWS, wide), 1) // HEAD, join(cross_lanes), 0.0),
                        axis=1, keepdims=True)
        back = there - here
        lane = iota((ROWS, BLK), 1)
        shift = 1
        while shift < BLK:
            back = back + jnp.where(lane < BLK - shift, pltpu.roll(back, BLK - shift, 1), 0.0)
            shift *= 2
        pre = pre_ref[:, tk]
        size_total = (here / step_s[heads8(b), :] - rate * (back + cross))[0:heads]
        ddecay_s[:, tk] = size_total * sigmoid(pre)

    pass0, pass1 = (Z - 1) * (PU - 1), (Z - 1) * PU * (groups - 1)

    def reduce(s):
        less = max(1, PU - 1)
        r = jnp.clip(s - pass0, 0, max(0, pass1 - 1))
        k = jnp.where(s < pass0, s // less, lax.rem(r // PU, max(1, Z - 1)))
        q = jnp.where(s < pass0, 1 + lax.rem(s, less), (1 + r // (PU * max(1, Z - 1))) * PU + lax.rem(r, PU))
        k = jnp.where(s < pass0 + pass1, k, Z - 1)
        q = jnp.where(s < pass0 + pass1, q, 1 + jnp.maximum(s - pass0 - pass1, 0))
        zc = chunk_of(k)
        rows = piece_rows(q)
        mine = (X - 1) * Z + k
        total = part[mine, rows, :]
        for xi in range(X - 1):
            x_copy(xi * Z + k, q).wait_recv()
            total = total + xrecv[xi * Z + k, rows, :]
        part[mine, rows, :] = total

        @pl.when(upstream(zc))
        def _():
            z_arrival(zc, q).wait_recv()
            part[mine, rows, :] += zbuf[zc, rows, :]

        @pl.when((zc == z) & (z > 0))
        def _():
            z_arrival(Z, q).wait_recv()
            part[mine, rows, :] += zbuf[Z, rows, :]

        @pl.when(zc != z)
        def _():
            z_copy(k, q).start()

    REV, FWD = 0, groups
    decays = []
    for u in range(groups):
        decays.append(reverse(u))
        if u == 0:
            for m in range(LOADS):
                x_load(m).start()
    loads[3].wait()

    def inner(u):
        def body(b, carry):
            inner_grads(u, b)
            return carry
        return body

    lead = max(0, blocks - LOADS)
    lax.fori_loop(0, lead, inner(0), 0, unroll=4)
    pl.semaphore_wait(barrier, n - 1 + ntp - 1)
    for u in range(groups):
        row_start(REV + u, dstates[u, 0], decays[u])
    loads[4].wait()

    def project(m, carry):
        x_load(m).wait()
        rows = pl.ds(pl.multiple_of(m * XR, XR), XR)
        pre = jnp.dot(xv[rows, :], wv[...], preferred_element_type=F32).astype(BF).astype(F32)
        sig = sigmoid(pre)
        vals_s[rows, :] = pre * sig
        vslope_s[rows, :] = sig * (1.0 + pre * (1.0 - sig))

        inner_grads(0, lead + m)
        return carry

    met = 3
    lax.fori_loop(0, met, project, 0)
    for u in range(groups):
        row_finish(REV + u, True)
    lax.fori_loop(met, LOADS, project, 0)
    decayed = forward()
    for u in range(groups):
        row_start(FWD + u, states[u, blocks], decayed[:, lanes_of(u)])
    col_finish(REV, True, outgo_s, 0)
    correct(0)
    steps = Z * (NP - 1)
    early = min(2 * (Z - 1), X * Z, (Z - 1) * (PU - 1)) if groups > 1 else 0
    at_end = (z == 0) | (z == Z - 1)

    def quiet(t):
        pass

    def early_step(t):
        @pl.when(at_end & (t < early))
        def _():
            reduce(t)

    chunks(0, 0, Z, quiet)
    for u in range(groups):
        row_finish(FWD + u, False)
    chunks(0, Z, X * Z, quiet)
    for u in range(1, groups):
        lax.fori_loop(0, blocks, inner(u), 0, unroll=4)
        col_finish(REV + u, True, outgo_s, u)
        correct(u)
        chunks(u, 0, X * Z, early_step if u == 1 else quiet)

    def alone(s, carry):
        @pl.when(jnp.logical_not(at_end & (s < early)))
        def _():
            reduce(s)
        return carry

    near = (Z - 1) * X
    lax.fori_loop(0, near, last_rows, 0)
    lax.fori_loop(0, early, alone, 0)
    for u in range(groups):
        col_finish(FWD + u, False, income_s, u)

    def both(i, carry):
        for r in range(2):
            @pl.when(early + 2 * i + r < steps)
            def _(r=r):
                reduce(early + 2 * i + r)

        @pl.when(i == blocks // 4)
        def _():
            lax.fori_loop(near, Z * X, last_rows, 0)

        for r in range(2):
            grads_of(2 * i + r)
        return carry

    lax.fori_loop(0, blocks // 2, both, 0)
    outs = [local(dkey_s, dkey_hbm, o_sem.at[0]), local(dquery_s, dquery_hbm, o_sem.at[1]),
            local(dgate_s, dgate_hbm, o_sem.at[2]), local(ddecay_s, ddecay_hbm, o_sem.at[4])]
    for copy in outs:
        copy.start()
    def norm_copy(d):
        return remote(norms.at[tpi], norms.at[tpi], ns.at[d - 1], nr.at[d - 1], "tp", lax.rem(tpi + d, ntp))

    own = X * Z - 1
    squares = jnp.zeros((1, CD), F32)
    seen = early + blocks
    for u in range(groups):
        until = pass0 + pass1 + (u + 1) * PU - 1
        if seen < until:
            lax.fori_loop(seen, until, alone, 0)
            seen = until
        if u == 0:
            for xi in range(X - 1):
                xl_copy(xi).wait_recv()
                part[own, 0:PIECE, :] += xlast[xi]
        rows = part[own, lanes_of(u), :]
        squares = squares + jnp.sum(rows * rows, axis=0, keepdims=True)
        if u == groups - 1:
            norms[tpi] = jnp.broadcast_to(squares, (ROWS, CD))
            for d in range(1, ntp):
                norm_copy(d).start()
        wg_s[:, lanes_of(u)] = rows.T

    wcopy = local(wg_s, wgrad_hbm, o_sem.at[3])
    wcopy.start()

    for i in range(2 * groups):
        back = i < groups
        for d in range(1, X):
            row_copy(i, d).wait_send()
        for d in range(1, Z):
            @pl.when(sends_to(d, back))
            def _(i=i, d=d, back=back):
                col_copy(i, d, back).wait_send()

    def sent(t, carry):
        x_copy(t // (NP - 1), 1 + lax.rem(t, NP - 1)).wait_send()
        return carry

    def passed(t, carry):
        z_copy(t // (NP - 1), 1 + lax.rem(t, NP - 1)).wait_send()
        return carry

    def passed_last(i, carry):
        zl_copy((i // (Z - 1)) * Z + lax.rem(i, Z - 1)).wait_send()
        return carry

    lax.fori_loop(0, (X - 1) * Z * (NP - 1), sent, 0)
    lax.fori_loop(0, (Z - 1) * (NP - 1), passed, 0)
    lax.fori_loop(0, X * (Z - 1), passed_last, 0)
    for xi in range(X - 1):
        xl_copy(xi).wait_send()
    for d in range(1, ntp):
        got = remote(norms.at[tpi], norms.at[lax.rem(tpi + ntp - d, ntp)], ns.at[d - 1], nr.at[d - 1], "tp",
                     lax.rem(tpi + d, ntp))
        got.wait()
    total = norms[0]
    for i in range(1, ntp):
        total = total + norms[i]
    norm_s[...] = total[0:1]
    ncopy = local(norm_s, norm_hbm, o_sem.at[5])
    ncopy.start()
    for copy in outs:
        copy.wait()
    wcopy.wait()
    ncopy.wait()


def write(*refs):
    count = len(refs) // 2
    sem = refs[-1]
    copies = [pltpu.make_async_copy(refs[i], refs[count + i], sem.at[i]) for i in range(count)]
    for copy in copies:
        copy.start()
    for copy in copies:
        copy.wait()


def shards(block_input, value_weight, key_rows, query_rows, decay_pre, decay_log, gate_rows, out_grad):
    heads = decay_log.shape[0]
    tokens, depth = block_input.shape
    groups = key_rows.shape[1] // STATE
    wide, narrow = heads * HEAD, groups * STATE
    blocks = tokens // BLK
    n, ntp = lax.axis_size("sp"), lax.axis_size("tp")
    X = max(1, ntp // 2)
    if n % X:
        X = 1
    Z = n // X
    cd = depth // n
    gw = heads // groups * HEAD
    NP = wide // PIECE
    XO = max(1, X - 1)
    c = dict(heads=heads, ratio=heads // groups, blocks=blocks, n=n, ntp=ntp, X=X, Z=Z, cd=cd)
    hbm = pl.BlockSpec(memory_space=pl.ANY)
    vmem = pl.BlockSpec(memory_space=pltpu.VMEM)
    V = pltpu.VMEM
    dma = pltpu.SemaphoreType.DMA
    outs = pl.pallas_call(
        functools.partial(kernel, c),
        in_specs=[hbm, hbm, hbm, hbm, vmem, pl.BlockSpec(memory_space=pltpu.SMEM), hbm, hbm],
        out_specs=[hbm] * 6,
        out_shape=[
            V((tokens, narrow), F32), V((tokens, narrow), F32), V((heads, tokens), F32),
            V((tokens, wide), F32), V((cd, wide), F32), V((1, cd), F32),
        ],
        scratch_shapes=[
            V((tokens, depth), BF), V((depth, wide), BF), V((tokens, narrow), BF), V((tokens, narrow), BF),
            V((tokens, wide), BF), V((tokens, wide), BF),
            V((blocks * ROWS, BLK), F32), V((blocks * ROWS, BLK), F32), V((blocks * ROWS, BLK), F32),
            V((tokens, 2 * ROWS), F32), V((tokens, wide), F32), V((tokens, wide), BF),
            V((groups, blocks + 1, STATE, gw), F32), V((groups, blocks + 1, STATE, gw), F32),
            V((blocks, ROWS, wide), F32), V((blocks, ROWS, wide), F32), V((blocks, ROWS, wide), F32),
            V((tokens, wide), F32), V((tokens, wide), F32), V((tokens, wide), F32), V((tokens, wide), F32),
            V((tokens, wide), BF), V((tokens, wide), F32), V((tokens, narrow), F32), V((tokens, narrow), F32),
            V((wide, tokens), BF), V((X * Z, wide, cd), F32), V((XO * Z, wide, cd), F32),
            V((Z + 1, wide, cd), F32), V((X * (Z + 1), PIECE, cd), F32), V((XO, PIECE, cd), F32),
            V((2 * groups, X, STATE + ROWS, gw), F32), V((2 * groups, STATE + ROWS, gw), F32),
            V((2 * groups, Z - 1, STATE + ROWS, gw), F32),
            V((groups, STATE, gw), F32), V((groups, STATE, gw), F32), V((2 * groups, STATE + ROWS, gw), F32),
            V((cd, wide), F32), V((ntp, ROWS, cd), F32), V((heads, tokens), F32), V((1, cd), F32),
            dma((5,)), dma((LOADS,)),
            dma((2 * groups, XO)), dma((2 * groups, XO)), dma((2 * groups, Z - 1)), dma((2 * groups, Z - 1)),
            dma((XO * Z * NP,)), dma((XO * Z * NP,)), dma((Z * NP,)), dma(((Z + 1) * NP,)),
            dma((X * Z,)), dma((X * (Z + 1),)), dma((XO,)), dma((XO,)),
            dma((ntp - 1,)), dma((ntp - 1,)), dma((6,)),
        ],
        compiler_params=pltpu.CompilerParams(
            collective_id=0, has_side_effects=True, vmem_limit_bytes=60_000_000),
        name="mixer_back",
    )(block_input, value_weight, key_rows, query_rows, decay_pre, decay_log, gate_rows, out_grad)
    outs = pl.pallas_call(
        write,
        in_specs=[vmem] * len(outs),
        out_specs=[hbm] * len(outs),
        out_shape=[jax.ShapeDtypeStruct(o.shape, o.dtype) for o in outs],
        scratch_shapes=[dma((len(outs),))],
        compiler_params=pltpu.CompilerParams(vmem_limit_bytes=1 << 20),
        name="write_results",
    )(*outs)
    key_grad, query_grad, decay_grad, gate_grad, weight_grad, norm = outs
    return key_grad, query_grad, decay_grad, gate_grad, weight_grad, norm.reshape(cd)


def solution(mesh):
    in_specs = (
        P("sp", None),
        P(None, "tp"),
        P("sp", "tp"),
        P("sp", "tp"),
        P("tp", "sp"),
        P("tp"),
        P("sp", "tp"),
        P("sp", "tp"),
    )
    out_specs = (P("sp", "tp"), P("sp", "tp"), P("tp", "sp"), P("sp", "tp"), P("sp", "tp"), P("sp"))
    return jax.shard_map(shards, mesh=mesh, in_specs=in_specs, out_specs=out_specs, check_vma=False)
```

```python
import functools

import jax
import jax.numpy as jnp
from jax import lax
from jax.experimental import pallas as pl
from jax.experimental.pallas import tpu as pltpu
from jax.sharding import PartitionSpec as P

HEAD = 64
STATE = 64
BLK = 128
ROWS = 8
LOADS = 4
PIECE = 32

BF = jnp.bfloat16
F32 = jnp.float32
MESH = pl.DeviceIdType.MESH


def dot(a, b, ca, cb):
    return lax.dot_general(a, b, (((ca,), (cb,)), ((), ())), preferred_element_type=F32)


def iota(shape, dim):
    return lax.broadcasted_iota(jnp.int32, shape, dim)


def sigmoid(v):
    return 1.0 / (1.0 + jnp.exp(-v))


def thirds(q):
    hi = q.astype(BF).astype(F32)
    rest = q - hi
    mid = rest.astype(BF).astype(F32)
    return jnp.concatenate([hi, mid, rest - mid], axis=0).astype(BF)


def halves(q):
    hi = q.astype(BF)
    return hi, (q - hi.astype(F32)).astype(BF)


def by_blocks(a, count, width):
    if count == 1:
        return a
    lane = iota(a.shape, 1) // width
    return jnp.concatenate([jnp.where(lane == i, a, jnp.zeros_like(a)) for i in range(count)], axis=0)


def kernel(c, x_hbm, w_hbm, key_hbm, query_hbm, pre_ref, log_ref, gate_hbm, out_hbm,
           dkey_hbm, dquery_hbm, ddecay_hbm, dgate_hbm, wgrad_hbm, norm_hbm,
           xv, wv, kv, qv, gv, ov, run_s, runs_s, step_s, cols_s, grads_s, gfs_s, dstates, states,
           fac_s, after_s, ahead_s, vals_s, te_s, dval_s, vslope_s, vte_s, dgate_s, dkey_s, dquery_s,
           vgt_s, part, xrecv, zbuf, zlast, xlast, row_in, col_out, col_in, outgo_s, income_s, pass_s,
           wg_s, norms, ddecay_s, norm_s,
           in_sem, x_sem, row_ss, row_rs, col_ss, col_rs, xs, xr, zs, zr, zls, zlr, xls, xlr, ns, nr, o_sem):
    heads, ratio, blocks, n, ntp, X, Z = c["heads"], c["ratio"], c["blocks"], c["n"], c["ntp"], c["X"], c["Z"]
    groups = heads // ratio
    wide, narrow, CD = heads * HEAD, groups * STATE, c["cd"]
    gw = ratio * HEAD
    PU = gw // PIECE
    NP = groups * PU
    tokens = blocks * BLK
    me, tpi = lax.axis_index("sp"), lax.axis_index("tp")
    z, x = me // X, lax.rem(me, X)

    def local(src, dst, sem):
        return pltpu.make_async_copy(src, dst, sem)

    def remote(src, dst, ssem, rsem, axis, to):
        return pltpu.make_async_remote_copy(src, dst, ssem, rsem, device_id={axis: to}, device_id_type=MESH)

    loads = [local(gate_hbm, gv, in_sem.at[0]), local(out_hbm, ov, in_sem.at[1]),
             local(query_hbm, qv, in_sem.at[2]), local(key_hbm, kv, in_sem.at[3]),
             local(w_hbm, wv, in_sem.at[4])]
    for copy in loads:
        copy.start()
    XR = tokens // LOADS

    def x_load(m):
        rows = pl.ds(pl.multiple_of(m * XR, XR), XR)
        return local(x_hbm.at[rows, :], xv.at[rows, :], x_sem.at[m])

    barrier = pltpu.get_barrier_semaphore()
    for d in range(1, n):
        pl.semaphore_signal(barrier, inc=1, device_id={"sp": lax.rem(me + d, n)}, device_id_type=MESH)
    for d in range(1, ntp):
        pl.semaphore_signal(barrier, inc=1, device_id={"tp": lax.rem(tpi + d, ntp)}, device_id_type=MESH)

    head_row = iota((ROWS, BLK), 0)
    rate = jnp.zeros((ROWS, BLK), F32)
    for h in range(heads):
        rate = jnp.where(head_row == h, jnp.broadcast_to(log_ref[h], (ROWS, BLK)), rate)
    rate = jnp.where(head_row < heads, jnp.exp(rate), 0.0)
    run_s[...] = jnp.zeros_like(run_s)
    for b in range(blocks):
        run_s[b * ROWS:b * ROWS + heads, :] = pre_ref[:, b * BLK:(b + 1) * BLK]
    pre_all = run_s[...]
    step_all = jnp.maximum(pre_all, 0.0) + jnp.log1p(jnp.exp(-jnp.abs(pre_all)))
    step_s[...] = step_all
    lanes = iota((blocks * ROWS, BLK), 1)
    acc = -jnp.concatenate([rate] * blocks, axis=0) * step_all
    shift = 1
    while shift < BLK:
        acc = acc + jnp.where(lanes >= shift, pltpu.roll(acc, shift, 1), 0.0)
        shift *= 2
    run_s[...] = acc
    runs_all = acc - jnp.log(step_all)
    runs_s[...] = runs_all
    for b in range(blocks):
        rows = slice(b * ROWS, (b + 1) * ROWS)
        cols_s[b * BLK:(b + 1) * BLK, :] = jnp.concatenate([acc[rows], runs_all[rows]], axis=0).T

    spread = jnp.where((iota((3 * ROWS, wide), 0) & (ROWS - 1)) == iota((3 * ROWS, wide), 1) // HEAD,
                       1.0, 0.0).astype(BF)
    pick = jnp.where(iota((ROWS, wide), 0) == iota((ROWS, wide), 1) // HEAD, 1.0, 0.0).astype(BF)
    at_row, at_col = iota((BLK, BLK), 0), iota((BLK, BLK), 1)

    def toks(b):
        return pl.ds(pl.multiple_of(b * BLK, BLK), BLK)

    def heads8(b):
        return pl.ds(pl.multiple_of(b * ROWS, ROWS), ROWS)

    def lanes_of(u):
        return slice(u * gw, (u + 1) * gw)

    def placed(a, u):
        rows = [a if g == u else jnp.zeros_like(a) for g in range(groups)]
        return rows[0] if groups == 1 else jnp.concatenate(rows, axis=0)

    def from_start(b, u):
        return dot(thirds(jnp.exp(run_s[heads8(b), :])), spread[:, lanes_of(u)], 0, 0)

    def to_end(b):
        run, runs = run_s[heads8(b), :], runs_s[heads8(b), :]
        return dot(thirds(jnp.exp(run[:, BLK - 1:BLK] - runs)), spread, 0, 0)

    def row_copy(i, d):
        return remote(row_in.at[i, 0], row_in.at[i, d], row_ss.at[i, d - 1], row_rs.at[i, d - 1], "sp",
                      z * X + lax.rem(x + d, X))

    def col_copy(i, d, back):
        to = lax.rem(z + (Z - d if back else d), Z) * X + x
        return remote(col_out.at[i], col_in.at[i, d - 1], col_ss.at[i, d - 1], col_rs.at[i, d - 1], "sp", to)

    def sends_to(d, back):
        return (z >= d) if back else (z + d < Z)

    def hears_from(d, back):
        return (z + d < Z) if back else (z >= d)

    def row_start(i, state, decayed):
        row_in[i, 0, 0:STATE, :] = state
        row_in[i, 0, STATE:STATE + ROWS, :] = decayed
        for d in range(1, X):
            row_copy(i, d).start()

    def row_finish(i, back):
        for d in range(1, X):
            row_copy(i, d).wait_recv()
        acc, fac = jnp.zeros((STATE, gw), F32), jnp.ones((ROWS, gw), F32)
        mine, mine_fac = acc, fac
        for xx in (reversed(range(X)) if back else range(X)):
            mine = jnp.where(x == xx, acc, mine)
            mine_fac = jnp.where(x == xx, fac, mine_fac)
            item = row_in[i, lax.rem(x - xx + X, X)]
            acc = item[0:STATE] + acc * item[STATE:STATE + 1]
            fac = fac * item[STATE:STATE + ROWS]
        pass_s[i, 0:STATE, :] = mine
        pass_s[i, STATE:STATE + ROWS, :] = mine_fac
        col_out[i, 0:STATE, :] = acc
        col_out[i, STATE:STATE + ROWS, :] = fac
        for d in range(1, Z):
            @pl.when(sends_to(d, back))
            def _(d=d):
                col_copy(i, d, back).start()

    def col_finish(i, back, into, u):
        into[u] = pass_s[i, 0:STATE, :]
        for d in range(1, Z):
            @pl.when(hears_from(d, back))
            def _(d=d):
                col_copy(i, d, back).wait_recv()
                into[u] += col_in[i, d - 1, 0:STATE, :] * pass_s[i, STATE:STATE + 1, :]
                pass_s[i, STATE:STATE + ROWS, :] *= col_in[i, d - 1, STATE:STATE + ROWS, :]

    for copy in loads[:3]:
        copy.wait()
    for m in range(LOADS):
        x_load(m).start()

    def reverse(u):
        gs = lanes_of(u)
        dstates[u, blocks] = jnp.zeros((STATE, gw), F32)

        def body(i, decayed):
            b = blocks - 1 - i
            tk = toks(b)
            gate, cot = gv[tk, gs].astype(F32), ov[tk, gs].astype(F32)
            sig = sigmoid(gate)
            cs = cot * sig
            grads = cs * gate
            grads_s[tk, gs] = grads
            dgate_s[tk, gs] = cs * (1.0 + gate * (1.0 - sig))
            fs = from_start(b, u)
            gfs = (grads * fs).astype(BF)
            gfs_s[tk, gs] = gfs
            factor = fs[BLK - 1:BLK, :]
            fac_s[b, :, gs] = jnp.broadcast_to(factor, (ROWS, gw))
            after_s[b, :, gs] = decayed
            back = dot(qv[tk, :], gfs, 0, 0)[u * STATE:(u + 1) * STATE]
            dstates[u, b] = dstates[u, b + 1] * factor + back
            return decayed * factor

        return lax.fori_loop(0, blocks, body, jnp.ones((ROWS, gw), F32), unroll=4)

    def inner_grads(u, b):
        gs = lanes_of(u)
        tk = toks(b)
        run = run_s[heads8(b), :]
        key, query = kv[tk, :], qv[tk, :]
        te = te_s[tk, gs]
        mine = iota((BLK, narrow), 1) // STATE == u
        scores = dot(key, jnp.where(mine, query, jnp.zeros_like(query)), 1, 1)
        cols = cols_s[tk, :]
        outer = dot(key, placed(dstates[u, b + 1].astype(BF), u), 1, 0) * te
        weights = []
        for h in range(u * ratio, (u + 1) * ratio):
            decay = jnp.exp(jnp.where(at_col >= at_row, run[h:h + 1, :] - cols[:, ROWS + h:ROWS + h + 1], -1e30))
            weights.append((scores * decay).astype(BF))
        spread_grads = by_blocks(grads_s[tk, gs].astype(BF), ratio, HEAD)
        dval_s[tk, gs] = dot(jnp.concatenate(weights, axis=1), spread_grads, 1, 0) + outer

    def forward():
        for u in range(groups):
            states[u, 0] = jnp.zeros((STATE, gw), F32)

        def body(b, before):
            tk = toks(b)
            vte = (vals_s[tk, :] * te_s[tk, :]).astype(BF)
            vte_s[tk, :] = vte
            factor = fac_s[b]
            ahead_s[b] = before
            add = dot(kv[tk, :], vte, 0, 0)
            for u in range(groups):
                gs = lanes_of(u)
                states[u, b + 1] = states[u, b] * factor[0:1, gs] + add[u * STATE:(u + 1) * STATE, gs]
            return before * factor

        return lax.fori_loop(0, blocks, body, jnp.ones((ROWS, wide), F32), unroll=4)

    def correct(u):
        gs = lanes_of(u)

        def body(b, carry):
            tk = toks(b)
            extra = (outgo_s[u] * after_s[b, 0:1, gs]).astype(BF)
            dval = dval_s[tk, gs] + dot(kv[tk, :], placed(extra, u), 1, 0) * te_s[tk, gs]
            dval_s[tk, gs] = dval
            vgt_s[gs, tk] = (dval * vslope_s[tk, gs]).T.astype(BF)
            return carry

        lax.fori_loop(0, blocks, body, 0, unroll=4)

    def chunk_of(k):
        out = jnp.int32(0)
        for i in range(Z):
            order = sorted(range(Z), key=lambda zc: -abs(zc - i))
            here = jnp.int32(0)
            for kk in range(Z):
                here = jnp.where(k == kk, order[kk], here)
            out = jnp.where(z == i, here, out)
        return out

    def piece_rows(q):
        return pl.ds(pl.multiple_of(q * PIECE, PIECE), PIECE)

    def x_copy(t, q):
        to = z * X + lax.rem(x + 1 + t // Z, X)
        return remote(part.at[t, piece_rows(q), :], xrecv.at[t, piece_rows(q), :], xs.at[t * NP + q],
                      xr.at[t * NP + q], "sp", to)

    def z_next(zc):
        to = jnp.where(zc < z, z - 1, z + 1)
        slot = jnp.where((zc > z) & (zc == to), Z, zc)
        return lax.rem(to * X + x + n, n), slot

    def z_copy(k, q):
        to, slot = z_next(chunk_of(k))
        return remote(part.at[(X - 1) * Z + k, piece_rows(q), :], zbuf.at[slot, piece_rows(q), :],
                      zs.at[k * NP + q], zr.at[slot * NP + q], "sp", to)

    def z_arrival(slot, q):
        return remote(part.at[0, piece_rows(q), :], zbuf.at[slot, piece_rows(q), :], zs.at[q],
                      zr.at[slot * NP + q], "sp", lax.rem(me + X, n))

    def zl_copy(t):
        to, slot = z_next(chunk_of(lax.rem(t, Z)))
        at = (t // Z) * (Z + 1) + slot
        return remote(part.at[t, 0:PIECE, :], zlast.at[at], zls.at[t], zlr.at[at], "sp", to)

    def zl_arrival(at):
        return remote(part.at[0, 0:PIECE, :], zlast.at[at], zls.at[0], zlr.at[at], "sp", lax.rem(me + X, n))

    def xl_copy(xi):
        k = Z - 1
        return remote(part.at[xi * Z + k, 0:PIECE, :], xlast.at[xi], xls.at[xi], xlr.at[xi], "sp",
                      z * X + lax.rem(x + 1 + xi, X))

    def upstream(zc):
        return ((zc <= z) & (z < Z - 1)) | ((zc > z) & (z > 0))

    def chunks(u, low, high, beside):
        def body(t, carry):
            beside(t)
            k = lax.rem(t, Z)
            zc = chunk_of(k)
            dest = zc * X + lax.rem(x + 1 + t // Z, X)
            step = min(256, CD)
            for half in range(CD // step):
                cs = pl.ds(pl.multiple_of(dest * CD + half * step, 128), step)
                part[t, lanes_of(u), half * step:(half + 1) * step] = jnp.dot(
                    vgt_s[lanes_of(u), :], xv[:, cs], preferred_element_type=F32)

            @pl.when(t < (X - 1) * Z)
            def _():
                for q in range(u * PU, (u + 1) * PU):
                    if q > 0:
                        x_copy(t, q).start()

            if u == 0:
                @pl.when((zc != z) & jnp.logical_not(upstream(zc)))
                def _():
                    zl_copy(t).start()
            return carry

        lax.fori_loop(low, high, body, 0)

    def last_rows(i, carry):
        k = i // X
        xi = lax.rem(i, X)
        t = xi * Z + k
        zc = chunk_of(k)
        base = xi * (Z + 1)

        @pl.when(upstream(zc))
        def _():
            zl_arrival(base + zc).wait_recv()
            part[t, 0:PIECE, :] += zlast[base + zc]

        @pl.when((zc == z) & (z > 0))
        def _():
            zl_arrival(base + Z).wait_recv()
            part[t, 0:PIECE, :] += zlast[base + Z]

        @pl.when((zc != z) & upstream(zc))
        def _():
            zl_copy(t).start()

        @pl.when((zc == z) & (xi < X - 1))
        def _():
            xl_copy(xi).start()
        return carry

    def grads_of(b):
        tk = toks(b)
        key, query = kv[tk, :], qv[tk, :]
        grads, vals = grads_s[tk, :], vals_s[tk, :]
        grads_b, vals_b = grads.astype(BF), vals.astype(BF)
        run, runs = run_s[heads8(b), :], runs_s[heads8(b), :]
        cols = cols_s[tk, :]
        state, dstate, cross_lanes = [], [], []
        for u in range(groups):
            gs = lanes_of(u)
            before, factor = ahead_s[b, 0:1, gs], fac_s[b, 0:1, gs]
            state.append(placed((states[u, b] + before * income_s[u]).astype(BF), u))
            after = states[u, b + 1] + (before * factor) * income_s[u]
            down = dstates[u, b + 1] + after_s[b, 0:1, gs] * outgo_s[u]
            dstate.append(placed(down.astype(BF), u))
            cross_lanes.append(jnp.sum(after * down, axis=0, keepdims=True))
        join = (lambda v: v[0]) if groups == 1 else (lambda v: jnp.concatenate(v, axis=1))
        state_b, dstate_b = join(state), join(dstate)
        keys = by_blocks(key, groups, STATE)
        scores = dot(query, keys, 1, 1)
        pulled = dot(grads_b, by_blocks(vals_b, heads, HEAD), 1, 1)
        fs = dot(thirds(jnp.exp(run)), spread, 0, 0)
        outer = dot(query, state_b, 1, 0) * fs
        totals = []
        mixed = []
        for g in range(groups):
            weights, total = [], None
            for h in range(g * ratio, (g + 1) * ratio):
                decay = jnp.exp(jnp.where(at_row >= at_col, cols[:, h:h + 1] - runs[h:h + 1, :], -1e30))
                weights.append((scores[:, g * BLK:(g + 1) * BLK] * decay).astype(BF))
                item = pulled[:, h * BLK:(h + 1) * BLK] * decay
                total = item if total is None else total + item
            totals.append(total.astype(BF))
            gs = lanes_of(g)
            inner = dot(jnp.concatenate(weights, axis=1), by_blocks(vals_b[:, gs], ratio, HEAD), 1, 0)
            mixed.append(inner + outer[:, gs])
        mixed = join(mixed)
        dgate_s[tk, :] = mixed * dgate_s[tk, :]
        total = join(totals)
        dquery_s[tk, :] = dot(gfs_s[tk, :], state_b, 1, 1) + dot(total, keys, 1, 0)
        across = dot(total, query, 0, 0)
        dkey = dot(vte_s[tk, :], dstate_b, 1, 1)
        mine = across[0:BLK]
        for g in range(1, groups):
            mine = jnp.where(iota((BLK, narrow), 1) // STATE == g, across[g * BLK:(g + 1) * BLK], mine)
        dkey_s[tk, :] = dkey + mine
        there = sum(dot(pick, part_, 1, 1) for part_ in halves(grads * mixed))
        here = sum(dot(pick, part_, 1, 1) for part_ in halves(vals * dval_s[tk, :]))
        cross = jnp.sum(jnp.where(iota((ROWS, wide), 0) == iota((ROWS, wide), 1) // HEAD, join(cross_lanes), 0.0),
                        axis=1, keepdims=True)
        back = there - here
        lane = iota((ROWS, BLK), 1)
        shift = 1
        while shift < BLK:
            back = back + jnp.where(lane < BLK - shift, pltpu.roll(back, BLK - shift, 1), 0.0)
            shift *= 2
        pre = pre_ref[:, tk]
        size_total = (here / step_s[heads8(b), :] - rate * (back + cross))[0:heads]
        ddecay_s[:, tk] = size_total * sigmoid(pre)

    pass0, pass1 = (Z - 1) * (PU - 1), (Z - 1) * PU * (groups - 1)

    def reduce(s):
        less = max(1, PU - 1)
        r = jnp.clip(s - pass0, 0, max(0, pass1 - 1))
        k = jnp.where(s < pass0, s // less, lax.rem(r // PU, max(1, Z - 1)))
        q = jnp.where(s < pass0, 1 + lax.rem(s, less), (1 + r // (PU * max(1, Z - 1))) * PU + lax.rem(r, PU))
        k = jnp.where(s < pass0 + pass1, k, Z - 1)
        q = jnp.where(s < pass0 + pass1, q, 1 + jnp.maximum(s - pass0 - pass1, 0))
        zc = chunk_of(k)
        rows = piece_rows(q)
        mine = (X - 1) * Z + k
        total = part[mine, rows, :]
        for xi in range(X - 1):
            x_copy(xi * Z + k, q).wait_recv()
            total = total + xrecv[xi * Z + k, rows, :]
        part[mine, rows, :] = total

        @pl.when(upstream(zc))
        def _():
            z_arrival(zc, q).wait_recv()
            part[mine, rows, :] += zbuf[zc, rows, :]

        @pl.when((zc == z) & (z > 0))
        def _():
            z_arrival(Z, q).wait_recv()
            part[mine, rows, :] += zbuf[Z, rows, :]

        @pl.when(zc != z)
        def _():
            z_copy(k, q).start()

    REV, FWD = 0, groups
    decays = [reverse(u) for u in range(groups)]
    pl.semaphore_wait(barrier, n - 1 + ntp - 1)
    for u in range(groups):
        row_start(REV + u, dstates[u, 0], decays[u])
    for copy in loads[3:]:
        copy.wait()

    def inner(u):
        def body(b, carry):
            inner_grads(u, b)
            return carry
        return body

    def project(m, carry):
        x_load(m).wait()
        rows = pl.ds(pl.multiple_of(m * XR, XR), XR)
        pre = jnp.dot(xv[rows, :], wv[...], preferred_element_type=F32).astype(BF).astype(F32)
        sig = sigmoid(pre)
        vals_s[rows, :] = pre * sig
        vslope_s[rows, :] = sig * (1.0 + pre * (1.0 - sig))
        for i in range(blocks // LOADS):
            b = m * (blocks // LOADS) + i
            te_s[toks(b), :] = to_end(b)
            if i < beside:
                inner_grads(0, b)
        return carry

    beside = min(2, blocks // LOADS)
    met = LOADS // 2
    lax.fori_loop(0, met, project, 0)
    for u in range(groups):
        row_finish(REV + u, True)
    lax.fori_loop(met, LOADS, project, 0)
    decayed = forward()
    for u in range(groups):
        row_start(FWD + u, states[u, blocks], decayed[:, lanes_of(u)])

    def others(m, carry):
        for i in range(beside, blocks // LOADS):
            inner_grads(0, m * (blocks // LOADS) + i)
        return carry

    if beside < blocks // LOADS:
        lax.fori_loop(0, LOADS, others, 0, unroll=2)
    col_finish(REV, True, outgo_s, 0)
    correct(0)
    steps = Z * (NP - 1)
    early = min(2 * (Z - 1), X * Z, (Z - 1) * (PU - 1)) if groups > 1 else 0
    at_end = (z == 0) | (z == Z - 1)

    def quiet(t):
        pass

    def early_step(t):
        @pl.when(at_end & (t < early))
        def _():
            reduce(t)

    chunks(0, 0, Z, quiet)
    for u in range(groups):
        row_finish(FWD + u, False)
    chunks(0, Z, X * Z, quiet)
    for u in range(1, groups):
        lax.fori_loop(0, blocks, inner(u), 0, unroll=4)
        col_finish(REV + u, True, outgo_s, u)
        correct(u)
        chunks(u, 0, X * Z, early_step if u == 1 else quiet)

    def alone(s, carry):
        @pl.when(jnp.logical_not(at_end & (s < early)))
        def _():
            reduce(s)
        return carry

    near = (Z - 1) * X
    lax.fori_loop(0, near, last_rows, 0)
    lax.fori_loop(0, early, alone, 0)
    for u in range(groups):
        col_finish(FWD + u, False, income_s, u)

    def both(i, carry):
        for r in range(2):
            @pl.when(early + 2 * i + r < steps)
            def _(r=r):
                reduce(early + 2 * i + r)

        @pl.when(i == blocks // 4)
        def _():
            lax.fori_loop(near, Z * X, last_rows, 0)

        for r in range(2):
            grads_of(2 * i + r)
        return carry

    lax.fori_loop(0, blocks // 2, both, 0)
    outs = [local(dkey_s, dkey_hbm, o_sem.at[0]), local(dquery_s, dquery_hbm, o_sem.at[1]),
            local(dgate_s, dgate_hbm, o_sem.at[2]), local(ddecay_s, ddecay_hbm, o_sem.at[4])]
    for copy in outs:
        copy.start()
    def norm_copy(d):
        return remote(norms.at[tpi], norms.at[tpi], ns.at[d - 1], nr.at[d - 1], "tp", lax.rem(tpi + d, ntp))

    own = X * Z - 1
    squares = jnp.zeros((1, CD), F32)
    seen = early + blocks
    for u in range(groups):
        until = pass0 + pass1 + (u + 1) * PU - 1
        if seen < until:
            lax.fori_loop(seen, until, alone, 0)
            seen = until
        if u == 0:
            for xi in range(X - 1):
                xl_copy(xi).wait_recv()
                part[own, 0:PIECE, :] += xlast[xi]
        rows = part[own, lanes_of(u), :]
        squares = squares + jnp.sum(rows * rows, axis=0, keepdims=True)
        if u == groups - 1:
            norms[tpi] = jnp.broadcast_to(squares, (ROWS, CD))
            for d in range(1, ntp):
                norm_copy(d).start()
        wg_s[:, lanes_of(u)] = rows.T

    wcopy = local(wg_s, wgrad_hbm, o_sem.at[3])
    wcopy.start()

    for i in range(2 * groups):
        back = i < groups
        for d in range(1, X):
            row_copy(i, d).wait_send()
        for d in range(1, Z):
            @pl.when(sends_to(d, back))
            def _(i=i, d=d, back=back):
                col_copy(i, d, back).wait_send()

    def sent(t, carry):
        x_copy(t // (NP - 1), 1 + lax.rem(t, NP - 1)).wait_send()
        return carry

    def passed(t, carry):
        z_copy(t // (NP - 1), 1 + lax.rem(t, NP - 1)).wait_send()
        return carry

    def passed_last(i, carry):
        zl_copy((i // (Z - 1)) * Z + lax.rem(i, Z - 1)).wait_send()
        return carry

    lax.fori_loop(0, (X - 1) * Z * (NP - 1), sent, 0)
    lax.fori_loop(0, (Z - 1) * (NP - 1), passed, 0)
    lax.fori_loop(0, X * (Z - 1), passed_last, 0)
    for xi in range(X - 1):
        xl_copy(xi).wait_send()
    for d in range(1, ntp):
        got = remote(norms.at[tpi], norms.at[lax.rem(tpi + ntp - d, ntp)], ns.at[d - 1], nr.at[d - 1], "tp",
                     lax.rem(tpi + d, ntp))
        got.wait()
    total = norms[0]
    for i in range(1, ntp):
        total = total + norms[i]
    norm_s[...] = total[0:1]
    ncopy = local(norm_s, norm_hbm, o_sem.at[5])
    ncopy.start()
    for copy in outs:
        copy.wait()
    wcopy.wait()
    ncopy.wait()


def write(*refs):
    count = len(refs) // 2
    sem = refs[-1]
    copies = [pltpu.make_async_copy(refs[i], refs[count + i], sem.at[i]) for i in range(count)]
    for copy in copies:
        copy.start()
    for copy in copies:
        copy.wait()


def shards(block_input, value_weight, key_rows, query_rows, decay_pre, decay_log, gate_rows, out_grad):
    heads = decay_log.shape[0]
    tokens, depth = block_input.shape
    groups = key_rows.shape[1] // STATE
    wide, narrow = heads * HEAD, groups * STATE
    blocks = tokens // BLK
    n, ntp = lax.axis_size("sp"), lax.axis_size("tp")
    X = max(1, ntp // 2)
    if n % X:
        X = 1
    Z = n // X
    cd = depth // n
    gw = heads // groups * HEAD
    NP = wide // PIECE
    XO = max(1, X - 1)
    c = dict(heads=heads, ratio=heads // groups, blocks=blocks, n=n, ntp=ntp, X=X, Z=Z, cd=cd)
    hbm = pl.BlockSpec(memory_space=pl.ANY)
    vmem = pl.BlockSpec(memory_space=pltpu.VMEM)
    V = pltpu.VMEM
    dma = pltpu.SemaphoreType.DMA
    outs = pl.pallas_call(
        functools.partial(kernel, c),
        in_specs=[hbm, hbm, hbm, hbm, vmem, pl.BlockSpec(memory_space=pltpu.SMEM), hbm, hbm],
        out_specs=[hbm] * 6,
        out_shape=[
            V((tokens, narrow), F32), V((tokens, narrow), F32), V((heads, tokens), F32),
            V((tokens, wide), F32), V((cd, wide), F32), V((1, cd), F32),
        ],
        scratch_shapes=[
            V((tokens, depth), BF), V((depth, wide), BF), V((tokens, narrow), BF), V((tokens, narrow), BF),
            V((tokens, wide), BF), V((tokens, wide), BF),
            V((blocks * ROWS, BLK), F32), V((blocks * ROWS, BLK), F32), V((blocks * ROWS, BLK), F32),
            V((tokens, 2 * ROWS), F32), V((tokens, wide), F32), V((tokens, wide), BF),
            V((groups, blocks + 1, STATE, gw), F32), V((groups, blocks + 1, STATE, gw), F32),
            V((blocks, ROWS, wide), F32), V((blocks, ROWS, wide), F32), V((blocks, ROWS, wide), F32),
            V((tokens, wide), F32), V((tokens, wide), F32), V((tokens, wide), F32), V((tokens, wide), F32),
            V((tokens, wide), BF), V((tokens, wide), F32), V((tokens, narrow), F32), V((tokens, narrow), F32),
            V((wide, tokens), BF), V((X * Z, wide, cd), F32), V((XO * Z, wide, cd), F32),
            V((Z + 1, wide, cd), F32), V((X * (Z + 1), PIECE, cd), F32), V((XO, PIECE, cd), F32),
            V((2 * groups, X, STATE + ROWS, gw), F32), V((2 * groups, STATE + ROWS, gw), F32),
            V((2 * groups, Z - 1, STATE + ROWS, gw), F32),
            V((groups, STATE, gw), F32), V((groups, STATE, gw), F32), V((2 * groups, STATE + ROWS, gw), F32),
            V((cd, wide), F32), V((ntp, ROWS, cd), F32), V((heads, tokens), F32), V((1, cd), F32),
            dma((5,)), dma((LOADS,)),
            dma((2 * groups, XO)), dma((2 * groups, XO)), dma((2 * groups, Z - 1)), dma((2 * groups, Z - 1)),
            dma((XO * Z * NP,)), dma((XO * Z * NP,)), dma((Z * NP,)), dma(((Z + 1) * NP,)),
            dma((X * Z,)), dma((X * (Z + 1),)), dma((XO,)), dma((XO,)),
            dma((ntp - 1,)), dma((ntp - 1,)), dma((6,)),
        ],
        compiler_params=pltpu.CompilerParams(
            collective_id=0, has_side_effects=True, vmem_limit_bytes=60_000_000),
        name="mixer_back",
    )(block_input, value_weight, key_rows, query_rows, decay_pre, decay_log, gate_rows, out_grad)
    outs = pl.pallas_call(
        write,
        in_specs=[vmem] * len(outs),
        out_specs=[hbm] * len(outs),
        out_shape=[jax.ShapeDtypeStruct(o.shape, o.dtype) for o in outs],
        scratch_shapes=[dma((len(outs),))],
        compiler_params=pltpu.CompilerParams(vmem_limit_bytes=1 << 20),
        name="write_results",
    )(*outs)
    key_grad, query_grad, decay_grad, gate_grad, weight_grad, norm = outs
    return key_grad, query_grad, decay_grad, gate_grad, weight_grad, norm.reshape(cd)


def solution(mesh):
    in_specs = (
        P("sp", None),
        P(None, "tp"),
        P("sp", "tp"),
        P("sp", "tp"),
        P("tp", "sp"),
        P("tp"),
        P("sp", "tp"),
        P("sp", "tp"),
    )
    out_specs = (P("sp", "tp"), P("sp", "tp"), P("tp", "sp"), P("sp", "tp"), P("sp", "tp"), P("sp"))
    return jax.shard_map(shards, mesh=mesh, in_specs=in_specs, out_specs=out_specs, check_vma=False)
```

```python
import functools

import jax
import jax.numpy as jnp
from jax import lax
from jax.experimental import pallas as pl
from jax.experimental.pallas import tpu as pltpu
from jax.sharding import PartitionSpec as P

HEAD = 64
STATE = 64
BLK = 128
ROWS = 8
LOADS = 4
PIECE = 32

BF = jnp.bfloat16
F32 = jnp.float32
MESH = pl.DeviceIdType.MESH


def dot(a, b, ca, cb):
    return lax.dot_general(a, b, (((ca,), (cb,)), ((), ())), preferred_element_type=F32)


def iota(shape, dim):
    return lax.broadcasted_iota(jnp.int32, shape, dim)


def sigmoid(v):
    return 1.0 / (1.0 + jnp.exp(-v))


def thirds(q):
    hi = q.astype(BF).astype(F32)
    rest = q - hi
    mid = rest.astype(BF).astype(F32)
    return jnp.concatenate([hi, mid, rest - mid], axis=0).astype(BF)


def halves(q):
    hi = q.astype(BF)
    return hi, (q - hi.astype(F32)).astype(BF)


def by_blocks(a, count, width):
    if count == 1:
        return a
    lane = iota(a.shape, 1) // width
    return jnp.concatenate([jnp.where(lane == i, a, jnp.zeros_like(a)) for i in range(count)], axis=0)


def kernel(c, x_hbm, w_hbm, key_hbm, query_hbm, pre_ref, log_ref, gate_hbm, out_hbm,
           dkey_hbm, dquery_hbm, ddecay_hbm, dgate_hbm, wgrad_hbm, norm_hbm,
           xv, wv, kv, qv, gv, ov, run_s, runs_s, step_s, cols_s, grads_s, gfs_s, dstates, states,
           fac_s, after_s, ahead_s, vals_s, te_s, dval_s, vslope_s, vte_s, dgate_s, dkey_s, dquery_s,
           vgt_s, part, xrecv, zbuf, zlast, xlast, row_in, col_out, col_in, outgo_s, income_s, pass_s,
           wg_s, norms, ddecay_s, norm_s,
           in_sem, x_sem, row_ss, row_rs, col_ss, col_rs, xs, xr, zs, zr, zls, zlr, xls, xlr, ns, nr, o_sem):
    heads, ratio, blocks, n, ntp, X, Z = c["heads"], c["ratio"], c["blocks"], c["n"], c["ntp"], c["X"], c["Z"]
    groups = heads // ratio
    wide, narrow, CD = heads * HEAD, groups * STATE, c["cd"]
    gw = ratio * HEAD
    PU = gw // PIECE
    NP = groups * PU
    tokens = blocks * BLK
    me, tpi = lax.axis_index("sp"), lax.axis_index("tp")
    z, x = me // X, lax.rem(me, X)

    def local(src, dst, sem):
        return pltpu.make_async_copy(src, dst, sem)

    def remote(src, dst, ssem, rsem, axis, to):
        return pltpu.make_async_remote_copy(src, dst, ssem, rsem, device_id={axis: to}, device_id_type=MESH)

    loads = [local(gate_hbm, gv, in_sem.at[0]), local(out_hbm, ov, in_sem.at[1]),
             local(query_hbm, qv, in_sem.at[2]), local(key_hbm, kv, in_sem.at[3]),
             local(w_hbm, wv, in_sem.at[4])]
    for copy in loads:
        copy.start()
    XR = tokens // LOADS

    def x_load(m):
        rows = pl.ds(pl.multiple_of(m * XR, XR), XR)
        return local(x_hbm.at[rows, :], xv.at[rows, :], x_sem.at[m])

    barrier = pltpu.get_barrier_semaphore()
    for d in range(1, n):
        pl.semaphore_signal(barrier, inc=1, device_id={"sp": lax.rem(me + d, n)}, device_id_type=MESH)
    for d in range(1, ntp):
        pl.semaphore_signal(barrier, inc=1, device_id={"tp": lax.rem(tpi + d, ntp)}, device_id_type=MESH)

    head_row = iota((ROWS, BLK), 0)
    rate = jnp.zeros((ROWS, BLK), F32)
    for h in range(heads):
        rate = jnp.where(head_row == h, jnp.broadcast_to(log_ref[h], (ROWS, BLK)), rate)
    rate = jnp.where(head_row < heads, jnp.exp(rate), 0.0)
    run_s[...] = jnp.zeros_like(run_s)
    for b in range(blocks):
        run_s[b * ROWS:b * ROWS + heads, :] = pre_ref[:, b * BLK:(b + 1) * BLK]
    pre_all = run_s[...]
    step_all = jnp.maximum(pre_all, 0.0) + jnp.log1p(jnp.exp(-jnp.abs(pre_all)))
    step_s[...] = step_all
    lanes = iota((blocks * ROWS, BLK), 1)
    acc = -jnp.concatenate([rate] * blocks, axis=0) * step_all
    shift = 1
    while shift < BLK:
        acc = acc + jnp.where(lanes >= shift, pltpu.roll(acc, shift, 1), 0.0)
        shift *= 2
    run_s[...] = acc
    runs_all = acc - jnp.log(step_all)
    runs_s[...] = runs_all
    for b in range(blocks):
        rows = slice(b * ROWS, (b + 1) * ROWS)
        cols_s[b * BLK:(b + 1) * BLK, :] = jnp.concatenate([acc[rows], runs_all[rows]], axis=0).T

    spread = jnp.where((iota((3 * ROWS, wide), 0) & (ROWS - 1)) == iota((3 * ROWS, wide), 1) // HEAD,
                       1.0, 0.0).astype(BF)
    pick = jnp.where(iota((ROWS, wide), 0) == iota((ROWS, wide), 1) // HEAD, 1.0, 0.0).astype(BF)
    at_row, at_col = iota((BLK, BLK), 0), iota((BLK, BLK), 1)

    def toks(b):
        return pl.ds(pl.multiple_of(b * BLK, BLK), BLK)

    def heads8(b):
        return pl.ds(pl.multiple_of(b * ROWS, ROWS), ROWS)

    def lanes_of(u):
        return slice(u * gw, (u + 1) * gw)

    def placed(a, u):
        rows = [a if g == u else jnp.zeros_like(a) for g in range(groups)]
        return rows[0] if groups == 1 else jnp.concatenate(rows, axis=0)

    def from_start(b, u):
        return dot(thirds(jnp.exp(run_s[heads8(b), :])), spread[:, lanes_of(u)], 0, 0)

    def to_end(b):
        run, runs = run_s[heads8(b), :], runs_s[heads8(b), :]
        return dot(thirds(jnp.exp(run[:, BLK - 1:BLK] - runs)), spread, 0, 0)

    def row_copy(i, d):
        return remote(row_in.at[i, 0], row_in.at[i, d], row_ss.at[i, d - 1], row_rs.at[i, d - 1], "sp",
                      z * X + lax.rem(x + d, X))

    def col_copy(i, d, back):
        to = lax.rem(z + (Z - d if back else d), Z) * X + x
        return remote(col_out.at[i], col_in.at[i, d - 1], col_ss.at[i, d - 1], col_rs.at[i, d - 1], "sp", to)

    def sends_to(d, back):
        return (z >= d) if back else (z + d < Z)

    def hears_from(d, back):
        return (z + d < Z) if back else (z >= d)

    def row_start(i, state, decayed):
        row_in[i, 0, 0:STATE, :] = state
        row_in[i, 0, STATE:STATE + ROWS, :] = decayed
        for d in range(1, X):
            row_copy(i, d).start()

    def row_finish(i, back):
        for d in range(1, X):
            row_copy(i, d).wait_recv()
        acc, fac = jnp.zeros((STATE, gw), F32), jnp.ones((ROWS, gw), F32)
        mine, mine_fac = acc, fac
        for xx in (reversed(range(X)) if back else range(X)):
            mine = jnp.where(x == xx, acc, mine)
            mine_fac = jnp.where(x == xx, fac, mine_fac)
            item = row_in[i, lax.rem(x - xx + X, X)]
            acc = item[0:STATE] + acc * item[STATE:STATE + 1]
            fac = fac * item[STATE:STATE + ROWS]
        pass_s[i, 0:STATE, :] = mine
        pass_s[i, STATE:STATE + ROWS, :] = mine_fac
        col_out[i, 0:STATE, :] = acc
        col_out[i, STATE:STATE + ROWS, :] = fac
        for d in range(1, Z):
            @pl.when(sends_to(d, back))
            def _(d=d):
                col_copy(i, d, back).start()

    def col_finish(i, back, into, u):
        into[u] = pass_s[i, 0:STATE, :]
        for d in range(1, Z):
            @pl.when(hears_from(d, back))
            def _(d=d):
                col_copy(i, d, back).wait_recv()
                into[u] += col_in[i, d - 1, 0:STATE, :] * pass_s[i, STATE:STATE + 1, :]
                pass_s[i, STATE:STATE + ROWS, :] *= col_in[i, d - 1, STATE:STATE + ROWS, :]

    for copy in loads[:3]:
        copy.wait()
    for m in range(LOADS):
        x_load(m).start()

    def reverse(u):
        gs = lanes_of(u)
        dstates[u, blocks] = jnp.zeros((STATE, gw), F32)

        def body(i, decayed):
            b = blocks - 1 - i
            tk = toks(b)
            gate, cot = gv[tk, gs].astype(F32), ov[tk, gs].astype(F32)
            sig = sigmoid(gate)
            cs = cot * sig
            grads = cs * gate
            grads_s[tk, gs] = grads
            dgate_s[tk, gs] = cs * (1.0 + gate * (1.0 - sig))
            fs = from_start(b, u)
            gfs = (grads * fs).astype(BF)
            gfs_s[tk, gs] = gfs
            factor = fs[BLK - 1:BLK, :]
            fac_s[b, :, gs] = jnp.broadcast_to(factor, (ROWS, gw))
            after_s[b, :, gs] = decayed
            back = dot(qv[tk, :], gfs, 0, 0)[u * STATE:(u + 1) * STATE]
            dstates[u, b] = dstates[u, b + 1] * factor + back
            return decayed * factor

        return lax.fori_loop(0, blocks, body, jnp.ones((ROWS, gw), F32), unroll=8)

    def inner_grads(u, b):
        gs = lanes_of(u)
        tk = toks(b)
        run = run_s[heads8(b), :]
        key, query = kv[tk, :], qv[tk, :]
        te = te_s[tk, gs]
        mine = iota((BLK, narrow), 1) // STATE == u
        scores = dot(key, jnp.where(mine, query, jnp.zeros_like(query)), 1, 1)
        cols = cols_s[tk, :]
        outer = dot(key, placed(dstates[u, b + 1].astype(BF), u), 1, 0) * te
        weights = []
        for h in range(u * ratio, (u + 1) * ratio):
            decay = jnp.exp(jnp.where(at_col >= at_row, run[h:h + 1, :] - cols[:, ROWS + h:ROWS + h + 1], -1e30))
            weights.append((scores * decay).astype(BF))
        spread_grads = by_blocks(grads_s[tk, gs].astype(BF), ratio, HEAD)
        dval_s[tk, gs] = dot(jnp.concatenate(weights, axis=1), spread_grads, 1, 0) + outer

    def forward():
        for u in range(groups):
            states[u, 0] = jnp.zeros((STATE, gw), F32)

        def body(b, before):
            tk = toks(b)
            vte = (vals_s[tk, :] * te_s[tk, :]).astype(BF)
            vte_s[tk, :] = vte
            factor = fac_s[b]
            ahead_s[b] = before
            add = dot(kv[tk, :], vte, 0, 0)
            for u in range(groups):
                gs = lanes_of(u)
                states[u, b + 1] = states[u, b] * factor[0:1, gs] + add[u * STATE:(u + 1) * STATE, gs]
            return before * factor

        return lax.fori_loop(0, blocks, body, jnp.ones((ROWS, wide), F32), unroll=4)

    def correct(u):
        gs = lanes_of(u)

        def body(b, carry):
            tk = toks(b)
            extra = (outgo_s[u] * after_s[b, 0:1, gs]).astype(BF)
            dval = dval_s[tk, gs] + dot(kv[tk, :], placed(extra, u), 1, 0) * te_s[tk, gs]
            dval_s[tk, gs] = dval
            vgt_s[gs, tk] = (dval * vslope_s[tk, gs]).T.astype(BF)
            return carry

        lax.fori_loop(0, blocks, body, 0, unroll=8)

    def chunk_of(k):
        out = jnp.int32(0)
        for i in range(Z):
            order = sorted(range(Z), key=lambda zc: -abs(zc - i))
            here = jnp.int32(0)
            for kk in range(Z):
                here = jnp.where(k == kk, order[kk], here)
            out = jnp.where(z == i, here, out)
        return out

    def piece_rows(q):
        return pl.ds(pl.multiple_of(q * PIECE, PIECE), PIECE)

    def x_copy(t, q):
        to = z * X + lax.rem(x + 1 + t // Z, X)
        return remote(part.at[t, piece_rows(q), :], xrecv.at[t, piece_rows(q), :], xs.at[t * NP + q],
                      xr.at[t * NP + q], "sp", to)

    def z_next(zc):
        to = jnp.where(zc < z, z - 1, z + 1)
        slot = jnp.where((zc > z) & (zc == to), Z, zc)
        return lax.rem(to * X + x + n, n), slot

    def z_copy(k, q):
        to, slot = z_next(chunk_of(k))
        return remote(part.at[(X - 1) * Z + k, piece_rows(q), :], zbuf.at[slot, piece_rows(q), :],
                      zs.at[k * NP + q], zr.at[slot * NP + q], "sp", to)

    def z_arrival(slot, q):
        return remote(part.at[0, piece_rows(q), :], zbuf.at[slot, piece_rows(q), :], zs.at[q],
                      zr.at[slot * NP + q], "sp", lax.rem(me + X, n))

    def zl_copy(t):
        to, slot = z_next(chunk_of(lax.rem(t, Z)))
        at = (t // Z) * (Z + 1) + slot
        return remote(part.at[t, 0:PIECE, :], zlast.at[at], zls.at[t], zlr.at[at], "sp", to)

    def zl_arrival(at):
        return remote(part.at[0, 0:PIECE, :], zlast.at[at], zls.at[0], zlr.at[at], "sp", lax.rem(me + X, n))

    def xl_copy(xi):
        k = Z - 1
        return remote(part.at[xi * Z + k, 0:PIECE, :], xlast.at[xi], xls.at[xi], xlr.at[xi], "sp",
                      z * X + lax.rem(x + 1 + xi, X))

    def upstream(zc):
        return ((zc <= z) & (z < Z - 1)) | ((zc > z) & (z > 0))

    def chunks(u, low, high, beside):
        def body(t, carry):
            beside(t)
            k = lax.rem(t, Z)
            zc = chunk_of(k)
            dest = zc * X + lax.rem(x + 1 + t // Z, X)
            step = min(256, CD)
            for half in range(CD // step):
                cs = pl.ds(pl.multiple_of(dest * CD + half * step, 128), step)
                part[t, lanes_of(u), half * step:(half + 1) * step] = jnp.dot(
                    vgt_s[lanes_of(u), :], xv[:, cs], preferred_element_type=F32)

            @pl.when(t < (X - 1) * Z)
            def _():
                for q in range(u * PU, (u + 1) * PU):
                    if q > 0:
                        x_copy(t, q).start()

            if u == 0:
                @pl.when((zc != z) & jnp.logical_not(upstream(zc)))
                def _():
                    zl_copy(t).start()
            return carry

        lax.fori_loop(low, high, body, 0)

    def last_rows(i, carry):
        k = i // X
        xi = lax.rem(i, X)
        t = xi * Z + k
        zc = chunk_of(k)
        base = xi * (Z + 1)

        @pl.when(upstream(zc))
        def _():
            zl_arrival(base + zc).wait_recv()
            part[t, 0:PIECE, :] += zlast[base + zc]

        @pl.when((zc == z) & (z > 0))
        def _():
            zl_arrival(base + Z).wait_recv()
            part[t, 0:PIECE, :] += zlast[base + Z]

        @pl.when((zc != z) & upstream(zc))
        def _():
            zl_copy(t).start()

        @pl.when((zc == z) & (xi < X - 1))
        def _():
            xl_copy(xi).start()
        return carry

    def grads_of(b):
        tk = toks(b)
        key, query = kv[tk, :], qv[tk, :]
        grads, vals = grads_s[tk, :], vals_s[tk, :]
        grads_b, vals_b = grads.astype(BF), vals.astype(BF)
        run, runs = run_s[heads8(b), :], runs_s[heads8(b), :]
        cols = cols_s[tk, :]
        state, dstate, cross_lanes = [], [], []
        for u in range(groups):
            gs = lanes_of(u)
            before, factor = ahead_s[b, 0:1, gs], fac_s[b, 0:1, gs]
            state.append(placed((states[u, b] + before * income_s[u]).astype(BF), u))
            after = states[u, b + 1] + (before * factor) * income_s[u]
            down = dstates[u, b + 1] + after_s[b, 0:1, gs] * outgo_s[u]
            dstate.append(placed(down.astype(BF), u))
            cross_lanes.append(jnp.sum(after * down, axis=0, keepdims=True))
        join = (lambda v: v[0]) if groups == 1 else (lambda v: jnp.concatenate(v, axis=1))
        state_b, dstate_b = join(state), join(dstate)
        keys = by_blocks(key, groups, STATE)
        scores = dot(query, keys, 1, 1)
        pulled = dot(grads_b, by_blocks(vals_b, heads, HEAD), 1, 1)
        fs = dot(thirds(jnp.exp(run)), spread, 0, 0)
        outer = dot(query, state_b, 1, 0) * fs
        totals = []
        mixed = []
        for g in range(groups):
            weights, total = [], None
            for h in range(g * ratio, (g + 1) * ratio):
                decay = jnp.exp(jnp.where(at_row >= at_col, cols[:, h:h + 1] - runs[h:h + 1, :], -1e30))
                weights.append((scores[:, g * BLK:(g + 1) * BLK] * decay).astype(BF))
                item = pulled[:, h * BLK:(h + 1) * BLK] * decay
                total = item if total is None else total + item
            totals.append(total.astype(BF))
            gs = lanes_of(g)
            inner = dot(jnp.concatenate(weights, axis=1), by_blocks(vals_b[:, gs], ratio, HEAD), 1, 0)
            mixed.append(inner + outer[:, gs])
        mixed = join(mixed)
        dgate_s[tk, :] = mixed * dgate_s[tk, :]
        total = join(totals)
        dquery_s[tk, :] = dot(gfs_s[tk, :], state_b, 1, 1) + dot(total, keys, 1, 0)
        across = dot(total, query, 0, 0)
        dkey = dot(vte_s[tk, :], dstate_b, 1, 1)
        mine = across[0:BLK]
        for g in range(1, groups):
            mine = jnp.where(iota((BLK, narrow), 1) // STATE == g, across[g * BLK:(g + 1) * BLK], mine)
        dkey_s[tk, :] = dkey + mine
        there = sum(dot(pick, part_, 1, 1) for part_ in halves(grads * mixed))
        here = sum(dot(pick, part_, 1, 1) for part_ in halves(vals * dval_s[tk, :]))
        cross = jnp.sum(jnp.where(iota((ROWS, wide), 0) == iota((ROWS, wide), 1) // HEAD, join(cross_lanes), 0.0),
                        axis=1, keepdims=True)
        back = there - here
        lane = iota((ROWS, BLK), 1)
        shift = 1
        while shift < BLK:
            back = back + jnp.where(lane < BLK - shift, pltpu.roll(back, BLK - shift, 1), 0.0)
            shift *= 2
        pre = pre_ref[:, tk]
        size_total = (here / step_s[heads8(b), :] - rate * (back + cross))[0:heads]
        ddecay_s[:, tk] = size_total * sigmoid(pre)

    pass0, pass1 = (Z - 1) * (PU - 1), (Z - 1) * PU * (groups - 1)

    def reduce(s):
        less = max(1, PU - 1)
        r = jnp.clip(s - pass0, 0, max(0, pass1 - 1))
        k = jnp.where(s < pass0, s // less, lax.rem(r // PU, max(1, Z - 1)))
        q = jnp.where(s < pass0, 1 + lax.rem(s, less), (1 + r // (PU * max(1, Z - 1))) * PU + lax.rem(r, PU))
        k = jnp.where(s < pass0 + pass1, k, Z - 1)
        q = jnp.where(s < pass0 + pass1, q, 1 + jnp.maximum(s - pass0 - pass1, 0))
        zc = chunk_of(k)
        rows = piece_rows(q)
        mine = (X - 1) * Z + k
        total = part[mine, rows, :]
        for xi in range(X - 1):
            x_copy(xi * Z + k, q).wait_recv()
            total = total + xrecv[xi * Z + k, rows, :]
        part[mine, rows, :] = total

        @pl.when(upstream(zc))
        def _():
            z_arrival(zc, q).wait_recv()
            part[mine, rows, :] += zbuf[zc, rows, :]

        @pl.when((zc == z) & (z > 0))
        def _():
            z_arrival(Z, q).wait_recv()
            part[mine, rows, :] += zbuf[Z, rows, :]

        @pl.when(zc != z)
        def _():
            z_copy(k, q).start()

    REV, FWD = 0, groups
    decays = [reverse(u) for u in range(groups)]
    pl.semaphore_wait(barrier, n - 1 + ntp - 1)
    for u in range(groups):
        row_start(REV + u, dstates[u, 0], decays[u])
    for copy in loads[3:]:
        copy.wait()

    def inner(u):
        def body(b, carry):
            inner_grads(u, b)
            return carry
        return body

    def project(m, carry):
        x_load(m).wait()
        rows = pl.ds(pl.multiple_of(m * XR, XR), XR)
        pre = jnp.dot(xv[rows, :], wv[...], preferred_element_type=F32).astype(BF).astype(F32)
        sig = sigmoid(pre)
        vals_s[rows, :] = pre * sig
        vslope_s[rows, :] = sig * (1.0 + pre * (1.0 - sig))
        for i in range(blocks // LOADS):
            b = m * (blocks // LOADS) + i
            te_s[toks(b), :] = to_end(b)
            if i < beside:
                inner_grads(0, b)
        return carry

    beside = min(2, blocks // LOADS)
    met = LOADS // 2
    lax.fori_loop(0, met, project, 0)
    for u in range(groups):
        row_finish(REV + u, True)
    lax.fori_loop(met, LOADS, project, 0)
    decayed = forward()
    for u in range(groups):
        row_start(FWD + u, states[u, blocks], decayed[:, lanes_of(u)])

    def others(m, carry):
        for i in range(beside, blocks // LOADS):
            inner_grads(0, m * (blocks // LOADS) + i)
        return carry

    if beside < blocks // LOADS:
        lax.fori_loop(0, LOADS, others, 0, unroll=4)
    col_finish(REV, True, outgo_s, 0)
    correct(0)
    steps = Z * (NP - 1)
    early = min(2 * (Z - 1), X * Z, (Z - 1) * (PU - 1)) if groups > 1 else 0
    at_end = (z == 0) | (z == Z - 1)

    def quiet(t):
        pass

    def early_step(t):
        @pl.when(at_end & (t < early))
        def _():
            reduce(t)

    chunks(0, 0, Z, quiet)
    for u in range(groups):
        row_finish(FWD + u, False)
    chunks(0, Z, X * Z, quiet)
    for u in range(1, groups):
        lax.fori_loop(0, blocks, inner(u), 0, unroll=4)
        col_finish(REV + u, True, outgo_s, u)
        correct(u)
        chunks(u, 0, X * Z, early_step if u == 1 else quiet)

    def alone(s, carry):
        @pl.when(jnp.logical_not(at_end & (s < early)))
        def _():
            reduce(s)
        return carry

    near = (Z - 1) * X
    lax.fori_loop(0, near, last_rows, 0)
    lax.fori_loop(0, early, alone, 0)
    for u in range(groups):
        col_finish(FWD + u, False, income_s, u)

    def both(i, carry):
        for r in range(2):
            @pl.when(early + 2 * i + r < steps)
            def _(r=r):
                reduce(early + 2 * i + r)

        @pl.when(i == blocks // 4)
        def _():
            lax.fori_loop(near, Z * X, last_rows, 0)

        for r in range(2):
            grads_of(2 * i + r)
        return carry

    lax.fori_loop(0, blocks // 2, both, 0)
    outs = [local(dkey_s, dkey_hbm, o_sem.at[0]), local(dquery_s, dquery_hbm, o_sem.at[1]),
            local(dgate_s, dgate_hbm, o_sem.at[2]), local(ddecay_s, ddecay_hbm, o_sem.at[4])]
    for copy in outs:
        copy.start()
    def norm_copy(d):
        return remote(norms.at[tpi], norms.at[tpi], ns.at[d - 1], nr.at[d - 1], "tp", lax.rem(tpi + d, ntp))

    own = X * Z - 1
    squares = jnp.zeros((1, CD), F32)
    seen = early + blocks
    for u in range(groups):
        until = pass0 + pass1 + (u + 1) * PU - 1
        if seen < until:
            lax.fori_loop(seen, until, alone, 0)
            seen = until
        if u == 0:
            for xi in range(X - 1):
                xl_copy(xi).wait_recv()
                part[own, 0:PIECE, :] += xlast[xi]
        rows = part[own, lanes_of(u), :]
        squares = squares + jnp.sum(rows * rows, axis=0, keepdims=True)
        if u == groups - 1:
            norms[tpi] = jnp.broadcast_to(squares, (ROWS, CD))
            for d in range(1, ntp):
                norm_copy(d).start()
        wg_s[:, lanes_of(u)] = rows.T

    wcopy = local(wg_s, wgrad_hbm, o_sem.at[3])
    wcopy.start()

    for i in range(2 * groups):
        back = i < groups
        for d in range(1, X):
            row_copy(i, d).wait_send()
        for d in range(1, Z):
            @pl.when(sends_to(d, back))
            def _(i=i, d=d, back=back):
                col_copy(i, d, back).wait_send()

    def sent(t, carry):
        x_copy(t // (NP - 1), 1 + lax.rem(t, NP - 1)).wait_send()
        return carry

    def passed(t, carry):
        z_copy(t // (NP - 1), 1 + lax.rem(t, NP - 1)).wait_send()
        return carry

    def passed_last(i, carry):
        zl_copy((i // (Z - 1)) * Z + lax.rem(i, Z - 1)).wait_send()
        return carry

    lax.fori_loop(0, (X - 1) * Z * (NP - 1), sent, 0)
    lax.fori_loop(0, (Z - 1) * (NP - 1), passed, 0)
    lax.fori_loop(0, X * (Z - 1), passed_last, 0)
    for xi in range(X - 1):
        xl_copy(xi).wait_send()
    for d in range(1, ntp):
        got = remote(norms.at[tpi], norms.at[lax.rem(tpi + ntp - d, ntp)], ns.at[d - 1], nr.at[d - 1], "tp",
                     lax.rem(tpi + d, ntp))
        got.wait()
    total = norms[0]
    for i in range(1, ntp):
        total = total + norms[i]
    norm_s[...] = total[0:1]
    ncopy = local(norm_s, norm_hbm, o_sem.at[5])
    ncopy.start()
    for copy in outs:
        copy.wait()
    wcopy.wait()
    ncopy.wait()


def write(*refs):
    count = len(refs) // 2
    sem = refs[-1]
    copies = [pltpu.make_async_copy(refs[i], refs[count + i], sem.at[i]) for i in range(count)]
    for copy in copies:
        copy.start()
    for copy in copies:
        copy.wait()


def shards(block_input, value_weight, key_rows, query_rows, decay_pre, decay_log, gate_rows, out_grad):
    heads = decay_log.shape[0]
    tokens, depth = block_input.shape
    groups = key_rows.shape[1] // STATE
    wide, narrow = heads * HEAD, groups * STATE
    blocks = tokens // BLK
    n, ntp = lax.axis_size("sp"), lax.axis_size("tp")
    X = max(1, ntp // 2)
    if n % X:
        X = 1
    Z = n // X
    cd = depth // n
    gw = heads // groups * HEAD
    NP = wide // PIECE
    XO = max(1, X - 1)
    c = dict(heads=heads, ratio=heads // groups, blocks=blocks, n=n, ntp=ntp, X=X, Z=Z, cd=cd)
    hbm = pl.BlockSpec(memory_space=pl.ANY)
    vmem = pl.BlockSpec(memory_space=pltpu.VMEM)
    V = pltpu.VMEM
    dma = pltpu.SemaphoreType.DMA
    outs = pl.pallas_call(
        functools.partial(kernel, c),
        in_specs=[hbm, hbm, hbm, hbm, vmem, pl.BlockSpec(memory_space=pltpu.SMEM), hbm, hbm],
        out_specs=[hbm] * 6,
        out_shape=[
            V((tokens, narrow), F32), V((tokens, narrow), F32), V((heads, tokens), F32),
            V((tokens, wide), F32), V((cd, wide), F32), V((1, cd), F32),
        ],
        scratch_shapes=[
            V((tokens, depth), BF), V((depth, wide), BF), V((tokens, narrow), BF), V((tokens, narrow), BF),
            V((tokens, wide), BF), V((tokens, wide), BF),
            V((blocks * ROWS, BLK), F32), V((blocks * ROWS, BLK), F32), V((blocks * ROWS, BLK), F32),
            V((tokens, 2 * ROWS), F32), V((tokens, wide), F32), V((tokens, wide), BF),
            V((groups, blocks + 1, STATE, gw), F32), V((groups, blocks + 1, STATE, gw), F32),
            V((blocks, ROWS, wide), F32), V((blocks, ROWS, wide), F32), V((blocks, ROWS, wide), F32),
            V((tokens, wide), F32), V((tokens, wide), F32), V((tokens, wide), F32), V((tokens, wide), F32),
            V((tokens, wide), BF), V((tokens, wide), F32), V((tokens, narrow), F32), V((tokens, narrow), F32),
            V((wide, tokens), BF), V((X * Z, wide, cd), F32), V((XO * Z, wide, cd), F32),
            V((Z + 1, wide, cd), F32), V((X * (Z + 1), PIECE, cd), F32), V((XO, PIECE, cd), F32),
            V((2 * groups, X, STATE + ROWS, gw), F32), V((2 * groups, STATE + ROWS, gw), F32),
            V((2 * groups, Z - 1, STATE + ROWS, gw), F32),
            V((groups, STATE, gw), F32), V((groups, STATE, gw), F32), V((2 * groups, STATE + ROWS, gw), F32),
            V((cd, wide), F32), V((ntp, ROWS, cd), F32), V((heads, tokens), F32), V((1, cd), F32),
            dma((5,)), dma((LOADS,)),
            dma((2 * groups, XO)), dma((2 * groups, XO)), dma((2 * groups, Z - 1)), dma((2 * groups, Z - 1)),
            dma((XO * Z * NP,)), dma((XO * Z * NP,)), dma((Z * NP,)), dma(((Z + 1) * NP,)),
            dma((X * Z,)), dma((X * (Z + 1),)), dma((XO,)), dma((XO,)),
            dma((ntp - 1,)), dma((ntp - 1,)), dma((6,)),
        ],
        compiler_params=pltpu.CompilerParams(
            collective_id=0, has_side_effects=True, vmem_limit_bytes=60_000_000),
        name="mixer_back",
    )(block_input, value_weight, key_rows, query_rows, decay_pre, decay_log, gate_rows, out_grad)
    outs = pl.pallas_call(
        write,
        in_specs=[vmem] * len(outs),
        out_specs=[hbm] * len(outs),
        out_shape=[jax.ShapeDtypeStruct(o.shape, o.dtype) for o in outs],
        scratch_shapes=[dma((len(outs),))],
        compiler_params=pltpu.CompilerParams(vmem_limit_bytes=1 << 20),
        name="write_results",
    )(*outs)
    key_grad, query_grad, decay_grad, gate_grad, weight_grad, norm = outs
    return key_grad, query_grad, decay_grad, gate_grad, weight_grad, norm.reshape(cd)


def solution(mesh):
    in_specs = (
        P("sp", None),
        P(None, "tp"),
        P("sp", "tp"),
        P("sp", "tp"),
        P("tp", "sp"),
        P("tp"),
        P("sp", "tp"),
        P("sp", "tp"),
    )
    out_specs = (P("sp", "tp"), P("sp", "tp"), P("tp", "sp"), P("sp", "tp"), P("sp", "tp"), P("sp"))
    return jax.shard_map(shards, mesh=mesh, in_specs=in_specs, out_specs=out_specs, check_vma=False)
```
